32 devices in a mesh: rep: 2 (over x), fs: 8 (over z, y), tp: 2 (over core).
Axes of the slice: x: 2, y: 2, z: 4, core: 2. Of those that a mesh axis runs over, the one named last changes fastest.
Arguments:
- x_late: bfloat16 [2048, 2048], P(('rep', 'fs')), parts along dimension 0, may hold values from -6 to 6
- x_early: bfloat16 [2048, 2048], P(('rep', 'fs')), parts along dimension 0, may hold values from -6 to 6
- cotangent: bfloat16 [2048, 2048], P(('rep', 'fs')), parts along dimension 0, may hold values from -6 to 6
- pre_gain: float32 [2048], replicated, may hold values from 0.1 to 1.9
- post_gain: float32 [2048], replicated, may hold values from 0.1 to 1.9
- gate_weight: bfloat16 [2048, 3072], P('fs', 'tp'), may hold values from -0.125 to 0.125
- up_weight: bfloat16 [2048, 3072], P('fs', 'tp'), may hold values from -0.125 to 0.125
- down_weight: bfloat16 [2048, 3072], P('fs', 'tp'), may hold values from -0.109375 to 0.109375
- down_grad_sum: float32 [4096, 3072], P(('rep', 'fs'), 'tp'), parts along dimension 0, may hold values from -6 to 6
Outputs:
- y_late: bfloat16 [2048, 2048], P(('rep', 'fs')), parts along dimension 0
- dx_early: bfloat16 [2048, 2048], P(('rep', 'fs')), parts along dimension 0
- down_grad_out: float32 [4096, 3072], P(('rep', 'fs'), 'tp'), parts along dimension 0
The draws below stay inside these ranges and needn't reach their ends.
There are 2 independent parts, one for each index of `rep`. The reference program is written for one: setup_inputs(seed, part) draws one part's arguments, and reference() takes and returns one part's arrays. A program takes and returns all parts, laid end to end along the dimension named above; an argument that names none is the same for every part. Nothing has to cross between parts.
All inputs are finite; a program needn't handle non-finite values.
Results may differ from the reference program's by a relative error of at most 0.023.
Values may be sent and summed in bfloat16 or wider, within the bound.
A program may use at most 64 MiB of HBM per device.

```python
import jax
import jax.numpy as jnp
from jax import lax

D = 2048
FF = 3072
TOKENS = 1024
N_TP = 2


def strengthened(array, key, source, target, blocks, factor):
    owner, partner = [(jnp.arange(array.shape[position]) // (array.shape[position] // blocks)).reshape([-1 if axis == position else 1 for axis in range(array.ndim)]) for position in (source, target)]
    chosen = jax.random.permutation(key, blocks)[partner]
    strong = (owner == chosen) | (owner == (partner + blocks // 2) % blocks)
    return jnp.where(strong, factor * array, array)


def block_scale(own_key, dims, pieces, smallest, top_value):
    def one(position, parts):
        heights = jax.random.uniform(jax.random.fold_in(jax.random.fold_in(own_key, 6), position), (parts,), jnp.float32, smallest / len(pieces), top_value / len(pieces))
        return jnp.repeat(jnp.exp(heights), dims[position] // parts).reshape((-1,) + (1,) * (len(dims) - position - 1))

    level = one(*pieces[0])
    for cut in pieces[1:]:
        level = level * one(*cut)
    return level


def noise(key, dims, scale, most, shards=(), dtype=jnp.bfloat16):
    loudness = block_scale(key, dims, shards, -0.22, 0.18) if shards else 1.0
    result = jax.random.normal(key, dims, jnp.float32) * scale * loudness
    return jnp.minimum(jnp.maximum(result, -most), most).astype(dtype)


def gaussian_with(rng, dims, spread, most, pieces, heavy, held_as=jnp.bfloat16):
    result = spread * jax.random.normal(rng, dims, jnp.float32)
    if pieces:
        result = result * block_scale(rng, dims, pieces, -0.22, 0.18)
    return jnp.clip(strengthened(result, jax.random.fold_in(rng, 3), *heavy), -most, most).astype(held_as)


def setup_inputs(seed: int = 0, part: int = 0) -> dict:
    splits = jax.random.split(jax.random.key(seed), 10)
    part_keys = jax.random.split(jax.random.fold_in(splits[9], part), 10)
    return {
        "x_late": noise(part_keys[0], (TOKENS, D), 1.0, 6.0, ((0, 8),)),
        "x_early": noise(part_keys[1], (TOKENS, D), 1.0, 6.0, ((0, 8),)),
        "cotangent": gaussian_with(part_keys[2], (TOKENS, D), 1.0, 6.0, ((0, 8),), (0, 1, 8, 2.0)),
        "pre_gain": jnp.clip(1.0 + 0.18 * jax.random.normal(splits[3], (D,), jnp.float32), 0.1, 1.9),
        "post_gain": jnp.clip(1.0 + 0.18 * jax.random.normal(splits[4], (D,), jnp.float32), 0.1, 1.9),
        "gate_weight": noise(splits[5], (D, FF), D ** -0.5, 0.125, ((0, 8), (1, 2))),
        "up_weight": noise(splits[6], (D, FF), D ** -0.5, 0.125, ((0, 8), (1, 2))),
        "down_weight": noise(splits[7], (D, FF), FF ** -0.5, 0.109375, ((0, 8), (1, 2))),
        "down_grad_sum": noise(part_keys[8], (D, FF), 1.0, 6.0, ((0, 8), (1, 2)), jnp.float32),
    }


eps = 1e-06

def pre_norm(x, pre_gain):
    xf = x.astype(jnp.float32)
    scale = lax.rsqrt(lax.optimization_barrier(jnp.mean(xf * xf, axis=-1, keepdims=True)) + eps)
    return (xf, scale, (xf * scale * pre_gain).astype(jnp.bfloat16))

def block_sum(left, right, width):
    total = jnp.zeros((left.shape[0], right.shape[0]), jnp.float32)
    for block in range(N_TP):
        lo = block * width
        term = lax.dot_general(left[:, lo:lo + width], right[:, lo:lo + width], (((1,), (1,)), ((), ())), preferred_element_type=jnp.float32)
        term = lax.optimization_barrier(term.astype(jnp.bfloat16))
        total = total + term.astype(jnp.float32)
    return total

def forward_branch(normed, gate_weight, up_weight, down_weight):
    gate = jnp.dot(normed, gate_weight, preferred_element_type=jnp.float32)
    up = jnp.dot(normed, up_weight, preferred_element_type=jnp.float32)
    hidden = (jax.nn.silu(gate) * up).astype(jnp.bfloat16)
    branch = block_sum(hidden, down_weight, FF // N_TP)
    return (gate, up, hidden, branch)

def reference(x_late, x_early, cotangent, pre_gain, post_gain, gate_weight, up_weight, down_weight, down_grad_sum):
    width = FF // N_TP
    late_f, late_rs, late_norm = pre_norm(x_late, pre_gain)
    gate_l, up_l, hidden_l, branch_l = forward_branch(late_norm, gate_weight, up_weight, down_weight)
    late_rz = lax.rsqrt(lax.optimization_barrier(jnp.mean(branch_l * branch_l, axis=-1, keepdims=True)) + eps)
    y_late = (late_f + 0.5 * branch_l * late_rz * post_gain).astype(jnp.bfloat16)
    early_f, early_rs, early_norm = pre_norm(x_early, pre_gain)
    gate_e, up_e, hidden_e, branch_e = forward_branch(early_norm, gate_weight, up_weight, down_weight)
    early_rz = lax.rsqrt(lax.optimization_barrier(jnp.mean(branch_e * branch_e, axis=-1, keepdims=True)) + eps)
    cot_f = cotangent.astype(jnp.float32)
    dpost = 0.5 * cot_f * post_gain
    dbranch = early_rz * (dpost - branch_e * early_rz * early_rz * lax.optimization_barrier(jnp.mean(branch_e * dpost, axis=-1, keepdims=True)))
    dbranch = dbranch.astype(jnp.bfloat16)
    dhidden = jnp.dot(dbranch, down_weight, preferred_element_type=jnp.float32)
    sig = jax.nn.sigmoid(gate_e)
    dgate = (dhidden * up_e * sig * (1.0 + gate_e * (1.0 - sig))).astype(jnp.bfloat16)
    dup = (dhidden * gate_e * sig).astype(jnp.bfloat16)
    dnormed = jnp.zeros(x_early.shape, jnp.float32)
    for block in range(N_TP):
        lo = block * width
        term = lax.dot_general(dgate[:, lo:lo + width], gate_weight[:, lo:lo + width], (((1,), (1,)), ((), ())), preferred_element_type=jnp.float32)
        term = term + lax.dot_general(dup[:, lo:lo + width], up_weight[:, lo:lo + width], (((1,), (1,)), ((), ())), preferred_element_type=jnp.float32)
        term = lax.optimization_barrier(term.astype(jnp.bfloat16))
        dnormed = dnormed + term.astype(jnp.float32)
    gained = pre_gain * dnormed
    dx_early = cot_f + early_rs * (gained - early_f * early_rs * early_rs * lax.optimization_barrier(jnp.mean(early_f * gained, axis=-1, keepdims=True)))
    dx_early = dx_early.astype(jnp.bfloat16)
    down_grad_out = down_grad_sum + lax.dot_general(dbranch, hidden_e, (((0,), (0,)), ((), ())), preferred_element_type=jnp.float32)
    return (y_late, dx_early, down_grad_out)
```

```python
import functools
import itertools

import jax
import jax.numpy as jnp
from jax import lax
from jax.experimental import pallas as pl
from jax.experimental.pallas import tpu as pltpu
from jax.sharding import PartitionSpec as P

eps = 1e-06
F32, BF16 = jnp.float32, jnp.bfloat16
VMEM = pl.BlockSpec(memory_space=pltpu.VMEM)
DMA = pltpu.SemaphoreType.DMA


class Grid:
    def __init__(self, sizes):
        self.R, self.fs, self.tp = sizes
        self.fy = 2
        self.fz = self.fs // self.fy
        self.G = self.R * self.fy
        self.offsets = list(itertools.product(range(self.R), range(self.fy)))[1:]
        self.r, f, self.k = (lax.axis_index(n) for n in ("rep", "fs", "tp"))
        self.z, self.y = lax.div(f, self.fy), lax.rem(f, self.fy)
        self.g = self.r * self.fy + self.y

    def moved(self, o, sign=1):
        dr, dy = self.offsets[o]
        r = lax.rem(self.r + self.R + sign * dr, self.R)
        y = lax.rem(self.y + self.fy + sign * dy, self.fy)
        return r, y

    def index(self, o, sign=1):
        r, y = self.moved(o, sign)
        return r * self.fy + y

    def peer(self, o):
        r, y = self.moved(o)
        return {"rep": r, "fs": self.z * self.fy + y, "tp": self.k}

    def sibling_index(self, j):
        return lax.rem(self.k + j, self.tp)

    def sibling(self, j):
        return {"rep": self.r, "fs": self.z * self.fy + self.y, "tp": self.sibling_index(j)}

    def along(self, step):
        return lax.rem(self.z + self.fz + step, self.fz)

    def level(self, step):
        return {"rep": self.r, "fs": self.along(step) * self.fy + self.y, "tp": self.k}

    def barrier(self, group=False, pair=False, ring=False, levels=False):
        sem = pltpu.get_barrier_semaphore()
        targets = []
        if group:
            targets += [self.peer(o) for o in range(len(self.offsets))]
        if pair:
            targets += [self.sibling(j) for j in range(1, self.tp)]
        if levels:
            targets += [self.level(s) for s in range(1, self.fz)]
        elif ring:
            targets += [self.level(1), self.level(-1)]
        for t in targets:
            pl.semaphore_signal(sem, inc=1, device_id=t, device_id_type=pl.DeviceIdType.MESH)
        pl.semaphore_wait(sem, len(targets))


def push(src, dst, send, recv, to):
    copy = pltpu.make_async_remote_copy(
        src_ref=src, dst_ref=dst, send_sem=send, recv_sem=recv,
        device_id=to, device_id_type=pl.DeviceIdType.MESH,
    )
    copy.start()
    return copy


def ring_start(m, first, slot, sems, chunks):
    half, sent = m.fz // 2, {}
    orders = {0: list(range(chunks)), 1: list(range(chunks))[chunks // 2:] + list(range(chunks // 2))}

    def send(d, s, c):
        sign = 1 if d == 0 else -1
        block = m.along(-sign * (s - 1))
        src = first(c) if s == 1 else slot(block, c)
        i = (d * half + s - 1) * chunks + c
        sent[d, s, c] = push(src, slot(block, c), sems.at[0, i], sems.at[1, i], m.level(sign))

    return orders, send, sent


def ring_travels(m, d, s, c, chunks):
    half = m.fz // 2
    return s < half or (c < chunks // 2) == (d == 0)


def ring_rest(m, orders, send, sent, chunks):
    half = m.fz // 2
    waited = set()
    for s in range(2, half + 1):
        for i in range(chunks):
            for d in (0, 1):
                c = orders[d][i]
                if ring_travels(m, d, s, c, chunks):
                    sent[d, s - 1, c].wait_recv()
                    waited.add((d, s - 1, c))
                    send(d, s, c)

    def finish():
        for key, copy in sent.items():
            copy.wait_send()
            if key not in waited:
                copy.wait_recv()

    return finish


def group_gather_start(m, x, out, sems):
    return [
        push(x.at[m.k], out.at[m.g, m.k], sems.at[0, o], sems.at[1, o], m.peer(o))
        for o in range(len(m.offsets))
    ]


def group_gather_finish(m, copies, out, sems):
    n, passed = len(m.offsets), []
    for o, copy in enumerate(copies):
        copy.wait_recv()
        src = m.index(o, -1)
        for j in range(1, m.tp):
            i = n + o * (m.tp - 1) + j - 1
            passed.append(
                push(out.at[src, m.k], out.at[src, m.k], sems.at[0, i], sems.at[1, i], m.sibling(j))
            )
    for copy in copies:
        copy.wait_send()
    for copy in passed:
        copy.wait()


def first_kernel(sizes, w, x, wout, xout, ysem, zsem, gsem):
    m = Grid(sizes)
    m.barrier(group=True, pair=True, ring=True)
    f = m.z * m.fy + m.y
    nw = w.shape[1]
    chunks = m.fy * nw

    def where(z, c):
        e, i = divmod(c, nw)
        return wout.at[i, z * m.fy + lax.rem(m.y + e, m.fy)]

    def first(c):
        return w.at[m.g, c] if c < nw else where(m.z, c)

    ycopies = {}
    for i in range(nw):
        for e in range(1, m.fy):
            o = m.offsets.index((0, e))
            j = (e - 1) * nw + i
            ycopies[e, i] = push(w.at[m.index(o), i], wout.at[i, f], ysem.at[0, j], ysem.at[1, j], m.peer(o))
    orders, send, sent = ring_start(m, first, where, zsem, chunks)
    for c in range(nw):
        send(0, 1, c)
        send(1, 1, c)
    gathered = group_gather_start(m, x, xout, gsem)
    for i in range(nw):
        wout[i, f] = w[m.g, i]
    xout[m.g] = x[...]
    for c in range(nw, chunks):
        e, i = divmod(c, nw)
        back = (m.fy - e) % m.fy
        ycopies[back, i].wait_recv()
        send(0, 1, c)
        send(1, 1, c)
    group_gather_finish(m, gathered, xout, gsem)
    finish = ring_rest(m, orders, send, sent, chunks)
    finish()
    for copy in ycopies.values():
        copy.wait_send()


def scatter_start(m, p, rx, sems):
    n = len(m.offsets)
    copies = {}
    for o in list(range(n)) + [n]:
        block = m.g if o == n else m.index(o)
        for j in range(1, m.tp):
            i = o * (m.tp - 1) + j - 1
            copies[o, j] = push(
                p.at[block, m.sibling_index(j)], rx.at[j - 1, o], sems.at[0, i], sems.at[1, i], m.sibling(j)
            )
    return copies


def scatter_rest(m, p, out, rx, tx, rg, copies, sems, fill=lambda: None):
    n = len(m.offsets)
    base = (n + 1) * (m.tp - 1)

    def total(o):
        block = m.g if o == n else m.index(o)
        value = p[block, m.k].astype(F32)
        for j in range(1, m.tp):
            copies[o, j].wait_recv()
            value = value + rx[j - 1, o].astype(F32)
        return value

    sends = []
    for o in range(n):
        tx[o] = total(o).astype(BF16)
        sends.append(push(tx.at[o], rg.at[o], sems.at[0, base + o], sems.at[1, base + o], m.peer(o)))
    out[m.k] = total(n)
    fill()
    for o in range(n):
        sends[o].wait_recv()
        out[m.k] = out[m.k] + rg[o].astype(F32)
    passed = []
    for j in range(1, m.tp):
        i = base + n + j - 1
        passed.append(push(out.at[m.k], out.at[m.k], sems.at[0, i], sems.at[1, i], m.sibling(j)))
    for copy in copies.values():
        copy.wait_send()
    for copy in sends:
        copy.wait_send()
    for copy in passed:
        copy.wait()


def branch_kernel(sizes, p, h, out, hout, rx, tx, rg, sems, zsem):
    m = Grid(sizes)
    m.barrier(group=True, pair=True, ring=True)
    copies = scatter_start(m, p, rx, sems)
    chunks = m.G
    orders, send, sent = ring_start(m, lambda c: h.at[c], lambda z, c: hout.at[z, c], zsem, chunks)
    for i in range(chunks):
        for d in (0, 1):
            send(d, 1, orders[d][i])

    ends = []

    def fill():
        hout[m.z] = h[...]
        ends.append(ring_rest(m, orders, send, sent, chunks))

    scatter_rest(m, p, out, rx, tx, rg, copies, sems, fill)
    ends[0]()


def gather_kernel(sizes, x, out, sems):
    m = Grid(sizes)
    m.barrier(group=True, pair=True)
    copies = group_gather_start(m, x, out, sems)
    out[m.g] = x[...]
    group_gather_finish(m, copies, out, sems)


def back_kernel(sizes, p, d, out, dout, rx, tx, rg, sems, zsem):
    m = Grid(sizes)
    m.barrier(group=True, pair=True, levels=True)
    copies = scatter_start(m, p, rx, sems)
    steps = list(range(1, m.fz))
    across = {}
    for s in steps:
        across[s] = push(
            d.at[m.along(s), m.k], dout.at[m.z, m.k], zsem.at[0, s - 1], zsem.at[1, s - 1], m.level(s)
        )
    passed = []

    def fill():
        dout[m.z] = d[m.z]

    scatter_rest(m, p, out, rx, tx, rg, copies, sems, fill)
    for s in steps:
        across[s].wait_recv()
        src = m.along(-s)
        for j in range(1, m.tp):
            i = len(steps) + (s - 1) * (m.tp - 1) + j - 1
            passed.append(push(dout.at[src, m.k], dout.at[src, m.k], zsem.at[0, i], zsem.at[1, i], m.sibling(j)))
    for s in steps:
        across[s].wait_send()
    for copy in passed:
        copy.wait()


def exchange_kernel(sizes, w, out, sems):
    m = Grid(sizes)
    m.barrier(group=True)
    copies = [
        push(w.at[m.index(o)], out.at[m.g], sems.at[0, o], sems.at[1, o], m.peer(o))
        for o in range(len(m.offsets))
    ]
    out[m.g] = w[m.g]
    for copy in copies:
        copy.wait()


def call(kernel, sizes, ident, outs, scratch, *args):
    size = sum(a.size * a.dtype.itemsize for a in list(args) + list(outs))
    return pl.pallas_call(
        functools.partial(kernel, sizes),
        out_shape=outs,
        in_specs=[VMEM] * len(args),
        out_specs=[VMEM] * len(outs),
        scratch_shapes=scratch,
        compiler_params=pltpu.CompilerParams(
            collective_id=ident, has_side_effects=True, vmem_limit_bytes=56 * 1024 * 1024
        ),
        cost_estimate=pl.CostEstimate(flops=0, bytes_accessed=size, transcendentals=0),
    )(*args)


def pre_norm(x, pre_gain):
    xf = x.astype(F32)
    scale = lax.rsqrt(jnp.mean(xf * xf, axis=-1, keepdims=True) + eps)
    return (xf, scale, (xf * scale * pre_gain).astype(BF16))


def right_product(left, right):
    return lax.dot_general(left, right, (((1,), (1,)), ((), ())), preferred_element_type=F32)


def body(sizes, x_late, x_early, cotangent, pre_gain, post_gain, gate_weight, up_weight, down_weight,
         down_grad_sum):
    R, fs, tp = sizes
    fy = 2
    fz, G = fs // fy, R * fy
    rows, D = x_late.shape
    drows, width = gate_weight.shape
    part = width // G
    n = G - 1
    S = jax.ShapeDtypeStruct

    late_f, late_rs, late_norm = pre_norm(x_late, pre_gain)
    early_f, early_rs, early_norm = pre_norm(x_early, pre_gain)
    normed = jnp.concatenate([late_norm, early_norm], axis=0)
    c = 2 * rows // tp
    weights = jnp.stack([w.reshape(drows, G, part) for w in (gate_weight, up_weight, down_weight)])
    weights = weights.transpose(2, 0, 1, 3)
    ring = fz // 2
    wall, xall = call(
        first_kernel, sizes, 0,
        [S((3, fs, drows, part), BF16), S((G, tp, c, D), BF16)],
        [DMA((2, 3 * (fy - 1))), DMA((2, 2 * ring * 3 * fy)), DMA((2, n + n * (tp - 1)))],
        weights, normed.reshape(tp, c, D),
    )
    wall = wall.reshape(3, D, part)
    xall = xall.reshape(G * 2 * rows, D)
    gate = jnp.dot(xall, wall[0], preferred_element_type=F32)
    up = jnp.dot(xall, wall[1], preferred_element_type=F32)
    hidden = (jax.nn.silu(gate) * up).astype(BF16)
    partial_value = right_product(hidden, wall[2]).astype(BF16).reshape(G, tp, c, D)
    early_of = lambda a: a.reshape(G, 2, rows, part)[:, 1]
    hidden_e = early_of(hidden)

    def scatter_scratch(c):
        return [
            pltpu.VMEM((tp - 1, n + 1, c, D), BF16),
            pltpu.VMEM((n, c, D), BF16),
            pltpu.VMEM((n, c, D), BF16),
            DMA((2, (n + 1) * (tp - 1) + n + tp - 1)),
        ]

    branch, hall = call(
        branch_kernel, sizes, 1,
        [S((tp, c, D), F32), S((fz, G, rows, part), BF16)],
        scatter_scratch(c) + [DMA((2, 2 * ring * G))],
        partial_value, hidden_e,
    )
    branch = branch.reshape(2 * rows, D)
    branch_l, branch_e = branch[:rows], branch[rows:]
    late_rz = lax.rsqrt(jnp.mean(branch_l * branch_l, axis=-1, keepdims=True) + eps)
    y_late = (late_f + 0.5 * branch_l * late_rz * post_gain).astype(BF16)
    early_rz = lax.rsqrt(jnp.mean(branch_e * branch_e, axis=-1, keepdims=True) + eps)
    cot_f = cotangent.astype(F32)
    dpost = 0.5 * cot_f * post_gain
    dbranch = early_rz * (
        dpost - branch_e * early_rz * early_rz * jnp.mean(branch_e * dpost, axis=-1, keepdims=True)
    )
    ce = rows // tp
    (dall,) = call(
        gather_kernel, sizes, 2,
        [S((G, tp, ce, D), BF16)],
        [DMA((2, n + n * (tp - 1)))],
        dbranch.astype(BF16).reshape(tp, ce, D),
    )
    dall = dall.reshape(G * rows, D)
    dhidden = jnp.dot(dall, wall[2], preferred_element_type=F32)
    gate_e = early_of(gate).reshape(G * rows, part)
    up_e = early_of(up).reshape(G * rows, part)
    sig = jax.nn.sigmoid(gate_e)
    dgate = (dhidden * up_e * sig * (1.0 + gate_e * (1.0 - sig))).astype(BF16)
    dup = (dhidden * gate_e * sig).astype(BF16)
    dpartial = right_product(dgate, wall[0]) + right_product(dup, wall[1])
    dpartial = dpartial.astype(BF16).reshape(G, tp, ce, D)
    feats = D // fz
    spread = dall.reshape(tp, G * rows // tp, fz, feats).transpose(2, 0, 1, 3)
    dnormed, dfeat = call(
        back_kernel, sizes, 3,
        [S((tp, ce, D), F32), S((fz, tp, G * rows // tp, feats), BF16)],
        scatter_scratch(ce) + [DMA((2, (fz - 1) * tp))],
        dpartial, spread,
    )
    gained = pre_gain * dnormed.reshape(rows, D)
    dx_early = cot_f + early_rs * (
        gained - early_f * early_rs * early_rs * jnp.mean(early_f * gained, axis=-1, keepdims=True)
    )
    dx_early = dx_early.astype(BF16)
    dfeat = dfeat.reshape(fz, R, fy * rows, feats)
    hall = hall.reshape(fz, R, fy * rows, part)
    summed = jnp.stack([
        lax.dot_general(
            dfeat[:, r].reshape(fz * fy * rows, feats), hall[:, r].reshape(fz * fy * rows, part),
            (((0,), (0,)), ((), ())), preferred_element_type=F32,
        )
        for r in range(R)
    ])
    summed = summed.astype(BF16).reshape(G, drows, part)
    (owned,) = call(exchange_kernel, sizes, 4, [S((G, drows, part), BF16)], [DMA((2, n))], summed)
    owned = owned.transpose(1, 0, 2).reshape(drows, width)
    down_grad_out = down_grad_sum + owned.astype(F32)
    return (y_late, dx_early, down_grad_out)


def solution(mesh):
    sizes = tuple(mesh.shape[a] for a in ("rep", "fs", "tp"))
    in_specs = (
        P(("rep", "fs"), None),
        P(("rep", "fs"), None),
        P(("rep", "fs"), None),
        P(),
        P(),
        P("fs", "tp"),
        P("fs", "tp"),
        P("fs", "tp"),
        P(("rep", "fs"), "tp"),
    )
    out_specs = (P(("rep", "fs"), None), P(("rep", "fs"), None), P(("rep", "fs"), "tp"))
    return jax.shard_map(
        functools.partial(body, sizes), mesh=mesh, in_specs=in_specs, out_specs=out_specs, check_vma=False
    )
```

```python
import functools
import itertools

import jax
import jax.numpy as jnp
from jax import lax
from jax.experimental import pallas as pl
from jax.experimental.pallas import tpu as pltpu
from jax.sharding import PartitionSpec as P

eps = 1e-06
F32, BF16 = jnp.float32, jnp.bfloat16
VMEM = pl.BlockSpec(memory_space=pltpu.VMEM)
DMA = pltpu.SemaphoreType.DMA


class Grid:
    def __init__(self, sizes):
        self.R, self.fs, self.tp = sizes
        self.fy = 2
        self.fz = self.fs // self.fy
        self.G = self.R * self.fy
        self.offsets = list(itertools.product(range(self.R), range(self.fy)))[1:]
        self.r, f, self.k = (lax.axis_index(n) for n in ("rep", "fs", "tp"))
        self.z, self.y = lax.div(f, self.fy), lax.rem(f, self.fy)
        self.g = self.r * self.fy + self.y

    def moved(self, o, sign=1):
        dr, dy = self.offsets[o]
        r = lax.rem(self.r + self.R + sign * dr, self.R)
        y = lax.rem(self.y + self.fy + sign * dy, self.fy)
        return r, y

    def index(self, o, sign=1):
        r, y = self.moved(o, sign)
        return r * self.fy + y

    def peer(self, o):
        r, y = self.moved(o)
        return {"rep": r, "fs": self.z * self.fy + y, "tp": self.k}

    def sibling_index(self, j):
        return lax.rem(self.k + j, self.tp)

    def sibling(self, j):
        return {"rep": self.r, "fs": self.z * self.fy + self.y, "tp": self.sibling_index(j)}

    def along(self, step):
        return lax.rem(self.z + self.fz + step, self.fz)

    def level(self, step):
        return {"rep": self.r, "fs": self.along(step) * self.fy + self.y, "tp": self.k}

    def barrier(self, group=False, pair=False, ring=False, levels=False):
        sem = pltpu.get_barrier_semaphore()
        targets = []
        if group:
            targets += [self.peer(o) for o in range(len(self.offsets))]
        if pair:
            targets += [self.sibling(j) for j in range(1, self.tp)]
        if levels:
            targets += [self.level(s) for s in range(1, self.fz)]
        elif ring:
            targets += [self.level(1), self.level(-1)]
        for t in targets:
            pl.semaphore_signal(sem, inc=1, device_id=t, device_id_type=pl.DeviceIdType.MESH)
        pl.semaphore_wait(sem, len(targets))


class Copies:
    def __init__(self, sems):
        self.sems, self.used = sems, 0

    def push(self, src, dst, to):
        copy = pltpu.make_async_remote_copy(
            src_ref=src, dst_ref=dst, send_sem=self.sems.at[0, self.used], recv_sem=self.sems.at[1, self.used],
            device_id=to, device_id_type=pl.DeviceIdType.MESH,
        )
        self.used += 1
        copy.start()
        return copy


class Ring:
    def __init__(self, m, cp, first, slot, chunks):
        self.m, self.cp, self.first, self.slot = m, cp, first, slot
        self.order = {0: chunks, 1: chunks[len(chunks) // 2:] + chunks[:len(chunks) // 2]}
        self.fronts = {0: set(chunks[: len(chunks) // 2]), 1: set(chunks[len(chunks) // 2:])}
        self.half = m.fz // 2
        self.sent, self.arrived = {}, set()

    def send(self, d, s, c):
        sign = 1 if d == 0 else -1
        block = self.m.along(-sign * (s - 1))
        src = self.first(c) if s == 1 else self.slot(block, c)
        self.sent[d, s, c] = self.cp.push(src, self.slot(block, c), self.m.level(sign))

    def arrive(self, d, s, c):
        if (d, s, c) not in self.sent or (d, s, c) in self.arrived:
            return
        self.sent[d, s, c].wait_recv()
        self.arrived.add((d, s, c))
        if s + 1 < self.half or (s + 1 == self.half and c in self.fronts[d]):
            self.send(d, s + 1, c)

    def step(self, s, ds=(0, 1)):
        for i in range(len(self.order[0])):
            for d in ds:
                self.arrive(d, s, self.order[d][i])

    def finish(self):
        for copy in self.sent.values():
            copy.wait_send()


def stages(m):
    half = m.fz // 2
    out = [(0, 0, ())]
    for s in range(1, half):
        out += [(-s, s, (0,)), (s, s, (1,))]
    return out + [(half, half, (0, 1))]


class Scatter:
    def __init__(self, m, cp, p, rx, tx, rg, acc):
        self.m, self.cp, self.p, self.rx, self.tx, self.rg, self.acc = m, cp, p, rx, tx, rg, acc
        self.pair, self.far = {}, {}

    def start(self, t):
        m = self.m
        for j in range(1, m.tp):
            src = self.p.at[t, :, :, m.sibling_index(j)]
            self.pair[t, j] = self.cp.push(src, self.rx.at[j - 1, t], m.sibling(j))

    def middle(self, t):
        m, n = self.m, len(self.m.offsets)
        for j in range(1, m.tp):
            self.pair[t, j].wait_recv()

        def total(block):
            value = self.p[t, :, block, m.k].astype(F32)
            for j in range(1, m.tp):
                value = value + self.rx[j - 1, t, :, block].astype(F32)
            return value

        for o in range(n):
            self.tx[t, o] = total(m.index(o)).astype(BF16)
            self.far[t, o] = self.cp.push(self.tx.at[t, o], self.rg.at[t, o], m.peer(o))
        self.acc[t] = total(m.g)

    def end(self, t):
        n = len(self.m.offsets)
        for o in range(n):
            self.far[t, o].wait_recv()
        value = self.acc[t]
        for o in range(n):
            value = value + self.rg[t, o].astype(F32)
        self.acc[t] = value

    def finish(self):
        for copy in list(self.pair.values()) + list(self.far.values()):
            copy.wait_send()


def flat(v):
    return v.reshape(-1, v.shape[-1])


def dot(a, b, ca, cb):
    return lax.dot_general(a, b, (((ca,), (cb,)), ((), ())), preferred_element_type=F32)


def kernel(sizes, D, w, x, dpost, branch_out, dnormed_out, owned_out,
           wout, xout, gate, up, hid, hout, p, rx, tx, rg, acc, dall, dhid, dgate, dup, dz,
           q, qx, qt, qg, dacc, dw, sems):
    m = Grid(sizes)
    cp = Copies(sems)
    n, fy, tp, fz = len(m.offsets), m.fy, m.tp, m.fz
    m.barrier(group=True, pair=True, levels=True)
    f = m.z * fy + m.y

    def where(z, c):
        e, i = c
        return wout.at[i, z * fy + lax.rem(m.y + e, fy)]

    def first(c):
        return w.at[m.g, c[1]] if c[0] == 0 else where(m.z, c)

    ys = {}

    def trade(i):
        for e in range(1, fy):
            o = m.offsets.index((0, e))
            ys[e, i] = cp.push(w.at[m.index(o), i], wout.at[i, f], m.peer(o))

    ring_a = Ring(m, cp, first, where, [(e, i) for i in (0, 1) for e in range(fy)])
    ring_b = Ring(m, cp, first, where, [(e, 2) for e in range(fy)])
    trade(0)
    trade(1)
    for i in (0, 1):
        ring_a.send(0, 1, (0, i))
        ring_a.send(1, 1, (0, 1 - i))
    xs = {o: cp.push(x.at[m.k], xout.at[m.g, m.k], m.peer(o)) for o in range(n)}
    trade(2)
    for i in range(3):
        wout[i, f] = w[m.g, i]
    xout[m.g] = x[...]
    for e in range(1, fy):
        back = (fy - e) % fy
        for i in (0, 1):
            ys[back, i].wait_recv()
        for i in (0, 1):
            ring_a.send(0, 1, (e, i))
            ring_a.send(1, 1, (e, 1 - i))
    for i in (0, 1):
        ring_a.arrive(0, 1, (0, i))
        ring_a.arrive(1, 1, (0, 1 - i))
    passed = []

    def spread(copies, out):
        for o in copies:
            copies[o].wait_recv()
            src = m.index(o, -1)
            for j in range(1, tp):
                passed.append(cp.push(out.at[src, m.k], out.at[src, m.k], m.sibling(j)))

    spread(xs, xout)
    ring_a.step(1)
    for e in range(fy):
        if e:
            ys[(fy - e) % fy, 2].wait_recv()
        for d in (0, 1):
            ring_b.send(d, 1, (e, 2))
    for copy in passed:
        copy.wait()
    passed.clear()

    gate[...] = jnp.zeros_like(gate)
    up[...] = jnp.zeros_like(up)
    for dist, s, ds in stages(m):
        for d in ds:
            ring_a.step(s, (d,))
        zt = m.along(dist)
        for e in range(fy):
            block = zt * fy + e

            def add(i, carry, block=block):
                rows = flat(xout[i, :, block])
                gate[i] += dot(rows, wout[0, block], 1, 0)
                up[i] += dot(rows, wout[1, block], 1, 0)
                return carry

            lax.fori_loop(0, m.G, add, 0)

    def activate(i, carry):
        v = gate[i]
        hid[i] = (v * (1.0 / (1.0 + jnp.exp(-v))) * up[i]).astype(BF16)
        return carry

    lax.fori_loop(0, m.G, activate, 0)
    ce = x.shape[2] // 2
    for t in range(tp):
        hout[m.z, t] = hid[:, (2 * t + 1) * ce:(2 * t + 2) * ce]
    ring_h = Ring(m, cp, lambda c: hout.at[m.z, c], lambda z, c: hout.at[z, c], list(range(tp)))

    sc = Scatter(m, cp, p, rx, tx, rg, acc)
    order = stages(m)
    for t, (dist, s, ds) in enumerate(order):
        for d in ds:
            ring_b.step(s, (d,))
        if t == len(order) - 1:
            for i in range(tp):
                for d in (0, 1):
                    ring_h.send(d, 1, ring_h.order[d][i])
        zt = m.along(dist)
        for e in range(fy):
            block = zt * fy + e

            def product(i, carry, block=block, e=e):
                p[t, e, i] = dot(hid[i], wout[2, block], 1, 1).astype(BF16).reshape(p.shape[3:])
                return carry

            lax.fori_loop(0, m.G, product, 0)
        sc.start(t)
        if t:
            sc.middle(t - 1)
    sc.middle(len(order) - 1)
    ssq = jnp.zeros((ce, 1), F32)
    mix = jnp.zeros((ce, 1), F32)
    for t, (dist, s, ds) in enumerate(order):
        sc.end(t)
        zt = m.along(dist)
        for e in range(fy):
            b = acc[t, e, ce:]
            ssq = ssq + jnp.sum(b * b, axis=-1, keepdims=True)
            mix = mix + jnp.sum(b * dpost[m.k, zt * fy + e], axis=-1, keepdims=True)
            branch_out[m.k, zt * fy + e] = acc[t, e, :ce]
    rz = lax.rsqrt(ssq / D + eps)
    factor = rz * rz * (mix / D)
    for t, (dist, s, ds) in enumerate(order):
        zt = m.along(dist)
        for e in range(fy):
            block = zt * fy + e
            dall[m.g, m.k, block] = (rz * (dpost[m.k, block] - acc[t, e, ce:] * factor)).astype(BF16)
    late = [cp.push(branch_out.at[m.k], branch_out.at[m.k], m.sibling(j)) for j in range(1, tp)]
    dg = {o: cp.push(dall.at[m.g, m.k], dall.at[m.g, m.k], m.peer(o)) for o in range(n)}
    own = [cp.push(dall.at[m.g, m.k], dall.at[m.g, m.k], m.sibling(j)) for j in range(1, tp)]
    ring_h.step(1)
    spread(dg, dall)
    across = {}
    for s in range(1, fz):
        src = dall.at[:, m.k, pl.ds(m.along(s) * fy, fy)]
        across[s] = cp.push(src, dz.at[m.z, m.k], m.level(s))
    for copy in passed + own:
        copy.wait()
    passed.clear()

    def back(i, carry):
        total = dot(flat(dall[i, :, 0]), wout[2, 0], 1, 0)
        for block in range(1, m.fs):
            total = total + dot(flat(dall[i, :, block]), wout[2, block], 1, 0)
        dhid[i] = total
        return carry

    lax.fori_loop(0, m.G, back, 0)

    def gates(i, carry):
        for t in range(tp):
            rows, mine = pl.ds((2 * t + 1) * ce, ce), pl.ds(t * ce, ce)
            g, dh = gate[i, rows], dhid[i, mine]
            sig = 1.0 / (1.0 + jnp.exp(-g))
            dgate[i, mine] = (dh * up[i, rows] * sig * (1.0 + g * (1.0 - sig))).astype(BF16)
            dup[i, mine] = (dh * g * sig).astype(BF16)
        return carry

    lax.fori_loop(0, m.G, gates, 0)
    dsc = Scatter(m, cp, q, qx, qt, qg, dacc)
    for t in range(fz):
        for e in range(fy):
            block = t * fy + e

            def terms(i, carry, block=block, e=e, t=t):
                v = dot(dgate[i], wout[0, block], 1, 1) + dot(dup[i], wout[1, block], 1, 1)
                q[t, e, i] = v.astype(BF16).reshape(q.shape[3:])
                return carry

            lax.fori_loop(0, m.G, terms, 0)
        dsc.start(t)
        if t:
            dsc.middle(t - 1)
    dsc.middle(fz - 1)
    for s in range(2, ring_h.half + 1):
        ring_h.step(s)
    dz[m.z] = jnp.stack([dall[:, t, pl.ds(m.z * fy, fy)] for t in range(tp)])
    for s in across:
        across[s].wait_recv()
        src = m.along(-s)
        for j in range(1, tp):
            passed.append(cp.push(dz.at[src, m.k], dz.at[src, m.k], m.sibling(j)))
    for t in range(fz):
        dsc.end(t)
        for e in range(fy):
            dnormed_out[m.k, t * fy + e] = dacc[t, e]
    last = [cp.push(dnormed_out.at[m.k], dnormed_out.at[m.k], m.sibling(j)) for j in range(1, tp)]
    for copy in passed:
        copy.wait()
    if fz == 1:
        ring_h.step(1)
    sends = []

    def gradient(r, e):
        a = dz[:, :, pl.ds(r * fy, fy), e]
        b = hout[:, :, pl.ds(r * fy, fy)]
        return dot(flat(a), flat(b), 0, 0).astype(BF16)

    for o in range(n):
        r, y = m.moved(o)
        dw[o] = gradient(r, y)
        sends.append(cp.push(dw.at[o], owned_out.at[m.g], m.peer(o)))
    owned_out[m.g] = gradient(m.r, m.y)
    for copy in sends + last + late:
        copy.wait()
    for copies in (xs, ys, dg, across):
        for copy in copies.values():
            copy.wait_send()
    for thing in (ring_a, ring_b, ring_h, sc, dsc):
        thing.finish()


def pre_norm(x, pre_gain):
    xf = x.astype(F32)
    scale = lax.rsqrt(jnp.mean(xf * xf, axis=-1, keepdims=True) + eps)
    return (xf, scale, (xf * scale * pre_gain).astype(BF16))


def body(sizes, x_late, x_early, cotangent, pre_gain, post_gain, gate_weight, up_weight, down_weight,
         down_grad_sum):
    R, fs, tp = sizes
    fy = 2
    fz, G = fs // fy, R * fy
    rows, D = x_late.shape
    drows, width = gate_weight.shape
    part = width // G
    n = G - 1
    ce = rows // tp
    c = 2 * ce
    S, V = jax.ShapeDtypeStruct, pltpu.VMEM

    late_f, late_rs, late_norm = pre_norm(x_late, pre_gain)
    early_f, early_rs, early_norm = pre_norm(x_early, pre_gain)
    blocks = lambda a: a.reshape(tp, ce, fs, drows).transpose(0, 2, 1, 3)
    rejoin = lambda a: a.transpose(0, 2, 1, 3).reshape(rows, D)
    normed = jnp.concatenate([blocks(late_norm), blocks(early_norm)], axis=2)
    weights = jnp.stack([w.reshape(drows, G, part) for w in (gate_weight, up_weight, down_weight)])
    weights = weights.transpose(2, 0, 1, 3)
    cot_f = cotangent.astype(F32)
    dpost = blocks(0.5 * cot_f * post_gain)
    ring = 2 * (fz // 2)
    count = (3 * (fy - 1) + ring * (3 * fy + tp) + 2 * (n + n * (tp - 1)) + 3 * (tp - 1)
             + 2 * fz * (tp - 1 + n) + (fz - 1) * tp + n)

    def scatter(c):
        return [
            V((fz, fy, G, tp, c, drows), BF16),
            V((tp - 1, fz, fy, G, c, drows), BF16),
            V((fz, n, fy, c, drows), BF16),
            V((fz, n, fy, c, drows), BF16),
            V((fz, fy, c, drows), F32),
        ]

    all_rows, early_rows = tp * c, tp * ce
    branch_l, dnormed, owned = pl.pallas_call(
        functools.partial(kernel, sizes, D),
        out_shape=[S((tp, fs, ce, drows), F32), S((tp, fs, ce, drows), F32), S((G, drows, part), BF16)],
        in_specs=[VMEM] * 3,
        out_specs=[VMEM] * 3,
        scratch_shapes=[
            V((3, fs, drows, part), BF16),
            V((G, tp, fs, c, drows), BF16),
            V((G, all_rows, part), F32),
            V((G, all_rows, part), F32),
            V((G, all_rows, part), BF16),
            V((fz, tp, G, ce, part), BF16),
        ] + scatter(c) + [
            V((G, tp, fs, ce, drows), BF16),
            V((G, early_rows, part), F32),
            V((G, early_rows, part), BF16),
            V((G, early_rows, part), BF16),
            V((fz, tp, G, fy, ce, drows), BF16),
        ] + scatter(ce) + [
            V((n, drows, part), BF16),
            DMA((2, count)),
        ],
        compiler_params=pltpu.CompilerParams(
            collective_id=0, has_side_effects=True, vmem_limit_bytes=60 * 1024 * 1024
        ),
    )(weights, normed, dpost)
    branch_l = rejoin(branch_l)
    late_rz = lax.rsqrt(jnp.mean(branch_l * branch_l, axis=-1, keepdims=True) + eps)
    y_late = (late_f + 0.5 * branch_l * late_rz * post_gain).astype(BF16)
    gained = pre_gain * rejoin(dnormed)
    dx_early = cot_f + early_rs * (
        gained - early_f * early_rs * early_rs * jnp.mean(early_f * gained, axis=-1, keepdims=True)
    )
    dx_early = dx_early.astype(BF16)
    owned = owned.transpose(1, 0, 2).reshape(drows, width)
    down_grad_out = down_grad_sum + owned.astype(F32)
    return (y_late, dx_early, down_grad_out)


def solution(mesh):
    sizes = tuple(mesh.shape[a] for a in ("rep", "fs", "tp"))
    in_specs = (
        P(("rep", "fs"), None),
        P(("rep", "fs"), None),
        P(("rep", "fs"), None),
        P(),
        P(),
        P("fs", "tp"),
        P("fs", "tp"),
        P("fs", "tp"),
        P(("rep", "fs"), "tp"),
    )
    out_specs = (P(("rep", "fs"), None), P(("rep", "fs"), None), P(("rep", "fs"), "tp"))
    return jax.shard_map(
        functools.partial(body, sizes), mesh=mesh, in_specs=in_specs, out_specs=out_specs, check_vma=False
    )
```

```python
import functools
import itertools

import jax
import jax.numpy as jnp
from jax import lax
from jax.experimental import pallas as pl
from jax.experimental.pallas import tpu as pltpu
from jax.sharding import PartitionSpec as P

eps = 1e-06
F32, BF16 = jnp.float32, jnp.bfloat16
VMEM = pl.BlockSpec(memory_space=pltpu.VMEM)
DMA = pltpu.SemaphoreType.DMA


class Grid:
    def __init__(self, sizes):
        self.R, self.fs, self.tp = sizes
        self.fy = 2
        self.fz = self.fs // self.fy
        self.G = self.R * self.fy
        self.offsets = list(itertools.product(range(self.R), range(self.fy)))[1:]
        self.r, f, self.k = (lax.axis_index(n) for n in ("rep", "fs", "tp"))
        self.z, self.y = lax.div(f, self.fy), lax.rem(f, self.fy)
        self.g = self.r * self.fy + self.y

    def moved(self, o, sign=1):
        dr, dy = self.offsets[o]
        r = lax.rem(self.r + self.R + sign * dr, self.R)
        y = lax.rem(self.y + self.fy + sign * dy, self.fy)
        return r, y

    def index(self, o, sign=1):
        r, y = self.moved(o, sign)
        return r * self.fy + y

    def peer(self, o):
        r, y = self.moved(o)
        return {"rep": r, "fs": self.z * self.fy + y, "tp": self.k}

    def sibling_index(self, j):
        return lax.rem(self.k + j, self.tp)

    def sibling(self, j):
        return {"rep": self.r, "fs": self.z * self.fy + self.y, "tp": self.sibling_index(j)}

    def along(self, step):
        return lax.rem(self.z + self.fz + step, self.fz)

    def level(self, step):
        return {"rep": self.r, "fs": self.along(step) * self.fy + self.y, "tp": self.k}

    def barrier(self, group=False, pair=False, ring=False, levels=False):
        sem = pltpu.get_barrier_semaphore()
        targets = []
        if group:
            targets += [self.peer(o) for o in range(len(self.offsets))]
        if pair:
            targets += [self.sibling(j) for j in range(1, self.tp)]
        if levels:
            targets += [self.level(s) for s in range(1, self.fz)]
        elif ring:
            targets += [self.level(1), self.level(-1)]
        for t in targets:
            pl.semaphore_signal(sem, inc=1, device_id=t, device_id_type=pl.DeviceIdType.MESH)
        pl.semaphore_wait(sem, len(targets))


class Copies:
    def __init__(self, sems):
        self.sems, self.used = sems, 0

    def push(self, src, dst, to):
        copy = pltpu.make_async_remote_copy(
            src_ref=src, dst_ref=dst, send_sem=self.sems.at[0, self.used], recv_sem=self.sems.at[1, self.used],
            device_id=to, device_id_type=pl.DeviceIdType.MESH,
        )
        self.used += 1
        copy.start()
        return copy


class Ring:
    def __init__(self, m, cp, first, slot, chunks):
        self.m, self.cp, self.first, self.slot = m, cp, first, slot
        self.order = {0: chunks, 1: chunks[len(chunks) // 2:] + chunks[:len(chunks) // 2]}
        self.fronts = {0: set(chunks[: len(chunks) // 2]), 1: set(chunks[len(chunks) // 2:])}
        self.half = m.fz // 2
        self.sent, self.arrived = {}, set()

    def send(self, d, s, c):
        sign = 1 if d == 0 else -1
        block = self.m.along(-sign * (s - 1))
        src = self.first(c) if s == 1 else self.slot(block, c)
        self.sent[d, s, c] = self.cp.push(src, self.slot(block, c), self.m.level(sign))

    def arrive(self, d, s, c):
        if (d, s, c) not in self.sent or (d, s, c) in self.arrived:
            return
        self.sent[d, s, c].wait_recv()
        self.arrived.add((d, s, c))
        if s + 1 < self.half or (s + 1 == self.half and c in self.fronts[d]):
            self.send(d, s + 1, c)

    def step(self, s, ds=(0, 1)):
        for i in range(len(self.order[0])):
            for d in ds:
                self.arrive(d, s, self.order[d][i])

    def finish(self):
        for copy in self.sent.values():
            copy.wait_send()


def stages(m):
    half = m.fz // 2
    out = [(0, 0, ())]
    for s in range(1, half):
        out += [(-s, s, (0,)), (s, s, (1,))]
    return out + [(half, half, (0, 1))]


class Scatter:
    def __init__(self, m, cp, p, rx, tx, rg, acc, place):
        self.m, self.cp, self.p, self.rx, self.tx, self.rg, self.acc = m, cp, p, rx, tx, rg, acc
        self.place = place
        self.pair, self.far = {}, {}

    def start(self, t):
        m = self.m
        for j in range(1, m.tp):
            src = self.p.at[t, :, :, m.sibling_index(j)]
            self.pair[t, j] = self.cp.push(src, self.rx.at[j - 1, t], m.sibling(j))

    def middle(self, t):
        m, n = self.m, len(self.m.offsets)
        for j in range(1, m.tp):
            self.pair[t, j].wait_recv()

        def total(block):
            value = self.p[t, :, block, m.k].astype(F32)
            for j in range(1, m.tp):
                value = value + self.rx[j - 1, t, :, block].astype(F32)
            return value

        for o in range(n):
            self.tx[t, o] = total(m.index(o)).astype(BF16)
            self.far[t, o] = self.cp.push(self.tx.at[t, o], self.rg.at[t, o], m.peer(o))
        self.acc[self.place(t)] = total(m.g)

    def end(self, t):
        n = len(self.m.offsets)
        for o in range(n):
            self.far[t, o].wait_recv()
        value = self.acc[self.place(t)]
        for o in range(n):
            value = value + self.rg[t, o].astype(F32)
        self.acc[self.place(t)] = value

    def finish(self):
        for copy in list(self.pair.values()) + list(self.far.values()):
            copy.wait_send()


def flat(v):
    return v.reshape(-1, v.shape[-1])


def dot(a, b, ca, cb):
    return lax.dot_general(a, b, (((ca,), (cb,)), ((), ())), preferred_element_type=F32)


def unit_scale(v):
    return lax.rsqrt(jnp.mean(v * v, axis=-1, keepdims=True) + eps)


def kernel(sizes, D, nw, *refs):
    ws, refs = refs[:nw], refs[nw:]
    (x_late, x_early, cot, pre_gain, post_gain, y_out, dx_out, owned_out,
     wout, xout, dpost, gate, up, hid, hout, p, rx, tx, rg, acc, dall, dhid, dgate, dup, dz,
           q, qx, qt, qg, dacc, dw, sems) = refs
    m = Grid(sizes)
    cp = Copies(sems)
    n, fy, tp, fz = len(m.offsets), m.fy, m.tp, m.fz
    m.barrier(group=True, pair=True, levels=True)
    f = m.z * fy + m.y
    rows, part = x_late.shape[0], wout.shape[-1]
    ce, drows = rows // tp, D // m.fs

    def weight(g, i):
        if nw == 1:
            return ws[0].at[g, i]
        return ws[i].at[:, pl.ds(pl.multiple_of(g * part, part), part)]

    def owned_at(g):
        if nw == 1:
            return owned_out.at[g]
        return owned_out.at[:, pl.ds(pl.multiple_of(g * part, part), part)]

    def columns(block):
        return slice(block * drows, (block + 1) * drows)

    def where(z, c):
        e, i = c
        return wout.at[i, z * fy + lax.rem(m.y + e, fy)]

    def first(c):
        return weight(m.g, c[1]) if c[0] == 0 else where(m.z, c)

    ys = {}

    def trade(i):
        for e in range(1, fy):
            o = m.offsets.index((0, e))
            ys[e, i] = cp.push(weight(m.index(o), i), wout.at[i, f], m.peer(o))

    ring_a = Ring(m, cp, first, where, [(e, i) for i in (0, 1) for e in range(fy)])
    ring_b = Ring(m, cp, first, where, [(e, 2) for e in range(fy)])
    trade(0)
    trade(1)
    for i in (0, 1):
        ring_a.send(0, 1, (0, i))
        ring_a.send(1, 1, (0, 1 - i))
    for t in range(tp):
        for place, ref in ((0, x_late), (ce, x_early)):
            v = ref[t * ce:(t + 1) * ce].astype(F32)
            v = (v * unit_scale(v) * pre_gain[...]).astype(BF16)
            for block in range(m.fs):
                xout[m.g, t, block, place:place + ce] = v[:, columns(block)]
    for i in range(3):
        wout[i, f] = weight(m.g, i)[...]
    xs = {o: cp.push(xout.at[m.g, m.k], xout.at[m.g, m.k], m.peer(o)) for o in range(n)}
    trade(2)
    mine = pl.ds(pl.multiple_of(m.k * ce, ce), ce)
    v = 0.5 * cot[mine].astype(F32) * post_gain[...]
    for block in range(m.fs):
        dpost[block] = v[:, columns(block)]
    for e in range(1, fy):
        back = (fy - e) % fy
        for i in (0, 1):
            ys[back, i].wait_recv()
        for i in (0, 1):
            ring_a.send(0, 1, (e, i))
            ring_a.send(1, 1, (e, 1 - i))
    for i in (0, 1):
        ring_a.arrive(0, 1, (0, i))
        ring_a.arrive(1, 1, (0, 1 - i))
    passed = []

    def spread(copies, out):
        for o in copies:
            copies[o].wait_recv()
            src = m.index(o, -1)
            for j in range(1, tp):
                passed.append(cp.push(out.at[src, m.k], out.at[src, m.k], m.sibling(j)))

    spread(xs, xout)
    ring_a.step(1)
    for e in range(fy):
        if e:
            ys[(fy - e) % fy, 2].wait_recv()
        for d in (0, 1):
            ring_b.send(d, 1, (e, 2))
    for copy in passed:
        copy.wait()
    passed.clear()

    gate[...] = jnp.zeros_like(gate)
    up[...] = jnp.zeros_like(up)
    for dist, s, ds in stages(m):
        for d in ds:
            ring_a.step(s, (d,))
        zt = m.along(dist)
        for e in range(fy):
            block = zt * fy + e

            def add(i, carry, block=block):
                rows = flat(xout[i, :, block])
                gate[i] += dot(rows, wout[0, block], 1, 0)
                up[i] += dot(rows, wout[1, block], 1, 0)
                return carry

            lax.fori_loop(0, m.G, add, 0)

    def activate(i, carry):
        v = gate[i]
        hid[i] = (v * (1.0 / (1.0 + jnp.exp(-v))) * up[i]).astype(BF16)
        return carry

    lax.fori_loop(0, m.G, activate, 0)
    for t in range(tp):
        hout[m.z, t] = hid[:, (2 * t + 1) * ce:(2 * t + 2) * ce]
    ring_h = Ring(m, cp, lambda c: hout.at[m.z, c], lambda z, c: hout.at[z, c], list(range(tp)))

    order = stages(m)
    sc = Scatter(m, cp, p, rx, tx, rg, acc, lambda t: m.along(order[t][0]))
    for t, (dist, s, ds) in enumerate(order):
        for d in ds:
            ring_b.step(s, (d,))
        if t == len(order) - 1:
            for i in range(tp):
                for d in (0, 1):
                    ring_h.send(d, 1, ring_h.order[d][i])
        zt = m.along(dist)
        for e in range(fy):
            block = zt * fy + e

            def product(i, carry, block=block, e=e):
                p[t, e, i] = dot(hid[i], wout[2, block], 1, 1).astype(BF16).reshape(p.shape[3:])
                return carry

            lax.fori_loop(0, m.G, product, 0)
        sc.start(t)
        if t:
            sc.middle(t - 1)
    sc.middle(len(order) - 1)
    for t in range(len(order)):
        sc.end(t)
    places = [divmod(block, fy) for block in range(m.fs)]

    def row_sum(term):
        return sum(jnp.sum(term(*place), axis=-1, keepdims=True) for place in places)

    rz = lax.rsqrt(row_sum(lambda t, e: acc[t, e, ce:] * acc[t, e, ce:]) / D + eps)
    mix = row_sum(lambda t, e: acc[t, e, ce:] * dpost[t * fy + e]) / D
    factor = rz * rz * mix
    for t, e in places:
        dall[m.g, m.k, t * fy + e] = (rz * (dpost[t * fy + e] - acc[t, e, ce:] * factor)).astype(BF16)
    dg = {o: cp.push(dall.at[m.g, m.k], dall.at[m.g, m.k], m.peer(o)) for o in range(n)}
    own = [cp.push(dall.at[m.g, m.k], dall.at[m.g, m.k], m.sibling(j)) for j in range(1, tp)]
    ring_h.step(1)
    late_rz = lax.rsqrt(row_sum(lambda t, e: acc[t, e, :ce] * acc[t, e, :ce]) / D + eps)
    for t, e in places:
        cols = columns(t * fy + e)
        v = 0.5 * acc[t, e, :ce] * late_rz * post_gain[:, cols]
        y_out[m.k, :, cols] = (x_late[mine, cols].astype(F32) + v).astype(BF16)
    spread(dg, dall)
    late = [cp.push(y_out.at[m.k], y_out.at[m.k], m.sibling(j)) for j in range(1, tp)]
    across = {}
    for s in range(1, fz):
        src = dall.at[:, m.k, pl.ds(m.along(s) * fy, fy)]
        across[s] = cp.push(src, dz.at[m.z, m.k], m.level(s))
    for copy in passed + own:
        copy.wait()
    passed.clear()

    def back(i, carry):
        total = dot(flat(dall[i, :, 0]), wout[2, 0], 1, 0)
        for block in range(1, m.fs):
            total = total + dot(flat(dall[i, :, block]), wout[2, block], 1, 0)
        dhid[i] = total
        return carry

    lax.fori_loop(0, m.G, back, 0)

    def gates(i, carry):
        for t in range(tp):
            its, to = pl.ds((2 * t + 1) * ce, ce), pl.ds(t * ce, ce)
            g, dh = gate[i, its], dhid[i, to]
            sig = 1.0 / (1.0 + jnp.exp(-g))
            dgate[i, to] = (dh * up[i, its] * sig * (1.0 + g * (1.0 - sig))).astype(BF16)
            dup[i, to] = (dh * g * sig).astype(BF16)
        return carry

    lax.fori_loop(0, m.G, gates, 0)
    dsc = Scatter(m, cp, q, qx, qt, qg, dacc, lambda t: t)
    for t in range(fz):
        for e in range(fy):
            block = t * fy + e

            def terms(i, carry, block=block, e=e, t=t):
                v = dot(dgate[i], wout[0, block], 1, 1) + dot(dup[i], wout[1, block], 1, 1)
                q[t, e, i] = v.astype(BF16).reshape(q.shape[3:])
                return carry

            lax.fori_loop(0, m.G, terms, 0)
        dsc.start(t)
        if t:
            dsc.middle(t - 1)
    dsc.middle(fz - 1)
    for s in range(2, ring_h.half + 1):
        ring_h.step(s)
    dz[m.z] = jnp.stack([dall[:, t, pl.ds(m.z * fy, fy)] for t in range(tp)])
    for s in across:
        across[s].wait_recv()
        src = m.along(-s)
        for j in range(1, tp):
            passed.append(cp.push(dz.at[src, m.k], dz.at[src, m.k], m.sibling(j)))
    for t in range(fz):
        dsc.end(t)
    xf = x_early[mine].astype(F32)
    rs = unit_scale(xf)
    gained = lambda t, e: dacc[t, e] * pre_gain[:, columns(t * fy + e)]
    mix = row_sum(lambda t, e: gained(t, e) * xf[:, columns(t * fy + e)]) / D
    factor = rs * rs * mix
    for t, e in places:
        cols = columns(t * fy + e)
        v = rs * (gained(t, e) - xf[:, cols] * factor)
        dx_out[m.k, :, cols] = (cot[mine, cols].astype(F32) + v).astype(BF16)
    last = [cp.push(dx_out.at[m.k], dx_out.at[m.k], m.sibling(j)) for j in range(1, tp)]
    for copy in passed:
        copy.wait()
    sends = []

    def gradient(r, e):
        a = dz[:, :, pl.ds(r * fy, fy), e]
        b = hout[:, :, pl.ds(r * fy, fy)]
        return dot(flat(a), flat(b), 0, 0).astype(BF16)

    for o in range(n):
        r, y = m.moved(o)
        dw[o] = gradient(r, y)
        sends.append(cp.push(dw.at[o], owned_at(m.g), m.peer(o)))
    owned_at(m.g)[...] = gradient(m.r, m.y)
    for copy in sends + last + late:
        copy.wait()
    for copies in (xs, ys, dg, across):
        for copy in copies.values():
            copy.wait_send()
    for thing in (ring_a, ring_b, ring_h, sc, dsc):
        thing.finish()


def body(sizes, x_late, x_early, cotangent, pre_gain, post_gain, gate_weight, up_weight, down_weight,
         down_grad_sum):
    R, fs, tp = sizes
    fy = 2
    fz, G = fs // fy, R * fy
    rows, D = x_late.shape
    drows, width = gate_weight.shape
    part = width // G
    n = G - 1
    ce = rows // tp
    c = 2 * ce
    S, V = jax.ShapeDtypeStruct, pltpu.VMEM

    weights = [gate_weight, up_weight, down_weight]
    aligned = part % 128 == 0
    if not aligned:
        weights = [jnp.stack([w.reshape(drows, G, part) for w in weights]).transpose(2, 0, 1, 3)]
    ring = 2 * (fz // 2)
    count = (3 * (fy - 1) + ring * (3 * fy + tp) + 2 * (n + n * (tp - 1)) + 3 * (tp - 1)
             + 2 * fz * (tp - 1 + n) + (fz - 1) * tp + n)

    def scatter(c):
        return [
            V((fz, fy, G, tp, c, drows), BF16),
            V((tp - 1, fz, fy, G, c, drows), BF16),
            V((fz, n, fy, c, drows), BF16),
            V((fz, n, fy, c, drows), BF16),
            V((fz, fy, c, drows), F32),
        ]

    all_rows, early_rows = tp * c, tp * ce
    y_late, dx_early, owned = pl.pallas_call(
        functools.partial(kernel, sizes, D, len(weights)),
        out_shape=[
            S((tp, ce, D), BF16), S((tp, ce, D), BF16),
            S((drows, width) if aligned else (G, drows, part), BF16),
        ],
        in_specs=[VMEM] * (len(weights) + 5),
        out_specs=[VMEM] * 3,
        scratch_shapes=[
            V((3, fs, drows, part), BF16),
            V((G, tp, fs, c, drows), BF16),
            V((fs, ce, drows), F32),
            V((G, all_rows, part), F32),
            V((G, all_rows, part), F32),
            V((G, all_rows, part), BF16),
            V((fz, tp, G, ce, part), BF16),
        ] + scatter(c) + [
            V((G, tp, fs, ce, drows), BF16),
            V((G, early_rows, part), F32),
            V((G, early_rows, part), BF16),
            V((G, early_rows, part), BF16),
            V((fz, tp, G, fy, ce, drows), BF16),
        ] + scatter(ce) + [
            V((n, drows, part), BF16),
            DMA((2, count)),
        ],
        compiler_params=pltpu.CompilerParams(
            collective_id=0, has_side_effects=True, vmem_limit_bytes=60 * 1024 * 1024
        ),
    )(*weights, x_late, x_early, cotangent, pre_gain.reshape(1, D), post_gain.reshape(1, D))
    if not aligned:
        owned = owned.transpose(1, 0, 2).reshape(drows, width)
    down_grad_out = down_grad_sum + owned.astype(F32)
    return (y_late.reshape(rows, D), dx_early.reshape(rows, D), down_grad_out)


def solution(mesh):
    sizes = tuple(mesh.shape[a] for a in ("rep", "fs", "tp"))
    in_specs = (
        P(("rep", "fs"), None),
        P(("rep", "fs"), None),
        P(("rep", "fs"), None),
        P(),
        P(),
        P("fs", "tp"),
        P("fs", "tp"),
        P("fs", "tp"),
        P(("rep", "fs"), "tp"),
    )
    out_specs = (P(("rep", "fs"), None), P(("rep", "fs"), None), P(("rep", "fs"), "tp"))
    return jax.shard_map(
        functools.partial(body, sizes), mesh=mesh, in_specs=in_specs, out_specs=out_specs, check_vma=False
    )
```

```python
import functools
import itertools

import jax
import jax.numpy as jnp
from jax import lax
from jax.experimental import pallas as pl
from jax.experimental.pallas import tpu as pltpu
from jax.sharding import PartitionSpec as P

eps = 1e-06
F32, BF16 = jnp.float32, jnp.bfloat16
VMEM = pl.BlockSpec(memory_space=pltpu.VMEM)
DMA = pltpu.SemaphoreType.DMA


class Grid:
    def __init__(self, sizes):
        self.R, self.fs, self.tp = sizes
        self.fy = 2
        self.fz = self.fs // self.fy
        self.G = self.R * self.fy
        self.offsets = list(itertools.product(range(self.R), range(self.fy)))[1:]
        self.r, f, self.k = (lax.axis_index(n) for n in ("rep", "fs", "tp"))
        self.z, self.y = lax.div(f, self.fy), lax.rem(f, self.fy)
        self.g = self.r * self.fy + self.y

    def moved(self, o, sign=1):
        dr, dy = self.offsets[o]
        r = lax.rem(self.r + self.R + sign * dr, self.R)
        y = lax.rem(self.y + self.fy + sign * dy, self.fy)
        return r, y

    def index(self, o, sign=1):
        r, y = self.moved(o, sign)
        return r * self.fy + y

    def peer(self, o):
        r, y = self.moved(o)
        return {"rep": r, "fs": self.z * self.fy + y, "tp": self.k}

    def sibling_index(self, j):
        return lax.rem(self.k + j, self.tp)

    def sibling(self, j):
        return {"rep": self.r, "fs": self.z * self.fy + self.y, "tp": self.sibling_index(j)}

    def along(self, step):
        return lax.rem(self.z + self.fz + step, self.fz)

    def level(self, step):
        return {"rep": self.r, "fs": self.along(step) * self.fy + self.y, "tp": self.k}

    def barrier(self, group=False, pair=False, ring=False, levels=False):
        sem = pltpu.get_barrier_semaphore()
        targets = []
        if group:
            targets += [self.peer(o) for o in range(len(self.offsets))]
        if pair:
            targets += [self.sibling(j) for j in range(1, self.tp)]
        if levels:
            targets += [self.level(s) for s in range(1, self.fz)]
        elif ring:
            targets += [self.level(1), self.level(-1)]
        for t in targets:
            pl.semaphore_signal(sem, inc=1, device_id=t, device_id_type=pl.DeviceIdType.MESH)
        pl.semaphore_wait(sem, len(targets))


class Copies:
    def __init__(self, sems):
        self.sems, self.used = sems, 0

    def push(self, src, dst, to):
        copy = pltpu.make_async_remote_copy(
            src_ref=src, dst_ref=dst, send_sem=self.sems.at[0, self.used], recv_sem=self.sems.at[1, self.used],
            device_id=to, device_id_type=pl.DeviceIdType.MESH,
        )
        self.used += 1
        copy.start()
        return copy


class Ring:
    def __init__(self, m, cp, first, slot, chunks):
        self.m, self.cp, self.first, self.slot = m, cp, first, slot
        self.order = {0: chunks, 1: chunks[len(chunks) // 2:] + chunks[:len(chunks) // 2]}
        self.fronts = {0: set(chunks[: len(chunks) // 2]), 1: set(chunks[len(chunks) // 2:])}
        self.half = m.fz // 2
        self.sent, self.arrived = {}, set()

    def send(self, d, s, c):
        sign = 1 if d == 0 else -1
        block = self.m.along(-sign * (s - 1))
        src = self.first(c) if s == 1 else self.slot(block, c)
        self.sent[d, s, c] = self.cp.push(src, self.slot(block, c), self.m.level(sign))

    def arrive(self, d, s, c):
        if (d, s, c) not in self.sent or (d, s, c) in self.arrived:
            return
        self.sent[d, s, c].wait_recv()
        self.arrived.add((d, s, c))
        if s + 1 < self.half or (s + 1 == self.half and c in self.fronts[d]):
            self.send(d, s + 1, c)

    def step(self, s, ds=(0, 1)):
        for i in range(len(self.order[0])):
            for d in ds:
                self.arrive(d, s, self.order[d][i])

    def finish(self):
        for copy in self.sent.values():
            copy.wait_send()


def stages(m):
    half = m.fz // 2
    out = [(0, 0, ())]
    for s in range(1, half):
        out += [(-s, s, (0,)), (s, s, (1,))]
    return out + [(half, half, (0, 1))]


class Scatter:
    def __init__(self, m, cp, p, rx, tx, rg, acc, place):
        self.m, self.cp, self.p, self.rx, self.tx, self.rg, self.acc = m, cp, p, rx, tx, rg, acc
        self.place = place
        self.pair, self.far = {}, {}

    def start(self, t):
        m = self.m
        for j in range(1, m.tp):
            src = self.p.at[t, :, :, m.sibling_index(j)]
            self.pair[t, j] = self.cp.push(src, self.rx.at[j - 1, t], m.sibling(j))

    def middle(self, t):
        m, n = self.m, len(self.m.offsets)
        for j in range(1, m.tp):
            self.pair[t, j].wait_recv()

        def total(block):
            value = self.p[t, :, block, m.k].astype(F32)
            for j in range(1, m.tp):
                value = value + self.rx[j - 1, t, :, block].astype(F32)
            return value

        for o in range(n):
            self.tx[t, o] = total(m.index(o)).astype(BF16)
            self.far[t, o] = self.cp.push(self.tx.at[t, o], self.rg.at[t, o], m.peer(o))
        self.acc[self.place(t)] = total(m.g)

    def end(self, t):
        n = len(self.m.offsets)
        for o in range(n):
            self.far[t, o].wait_recv()
        value = self.acc[self.place(t)]
        for o in range(n):
            value = value + self.rg[t, o].astype(F32)
        self.acc[self.place(t)] = value

    def finish(self):
        for copy in list(self.pair.values()) + list(self.far.values()):
            copy.wait_send()


def flat(v):
    return v.reshape(-1, v.shape[-1])


def dot(a, b, ca, cb):
    return lax.dot_general(a, b, (((ca,), (cb,)), ((), ())), preferred_element_type=F32)


def unit_scale(v):
    return lax.rsqrt(jnp.mean(v * v, axis=-1, keepdims=True) + eps)


def kernel(sizes, D, nw, *refs):
    ws, refs = refs[:nw], refs[nw:]
    (x_late, x_early, cot, pre_gain, post_gain, y_out, dx_out, owned_out,
     wout, xout, dpost, gate, up, hid, hout, p, rx, tx, rg, acc, dall, dhid, dgate, dup, dz,
           q, qx, qt, qg, dacc, dw, sems) = refs
    m = Grid(sizes)
    cp = Copies(sems)
    n, fy, tp, fz = len(m.offsets), m.fy, m.tp, m.fz
    m.barrier(group=True, pair=True, levels=True)
    f = m.z * fy + m.y
    rows, part = x_late.shape[0], wout.shape[-1]
    ce, drows = rows // tp, D // m.fs

    def weight(g, i):
        if nw == 1:
            return ws[0].at[g, i]
        return ws[i].at[:, pl.ds(pl.multiple_of(g * part, part), part)]

    def owned_at(g):
        if nw == 1:
            return owned_out.at[g]
        return owned_out.at[:, pl.ds(pl.multiple_of(g * part, part), part)]

    def columns(block):
        return slice(block * drows, (block + 1) * drows)

    def where(z, c):
        e, i = c
        return wout.at[i, z * fy + lax.rem(m.y + e, fy)]

    def first(c):
        return weight(m.g, c[1]) if c[0] == 0 else where(m.z, c)

    ys = {}

    def trade(i):
        for e in range(1, fy):
            o = m.offsets.index((0, e))
            ys[e, i] = cp.push(weight(m.index(o), i), wout.at[i, f], m.peer(o))

    ring_a = Ring(m, cp, first, where, [(e, i) for i in (0, 1) for e in range(fy)])
    ring_b = Ring(m, cp, first, where, [(e, 2) for e in range(fy)])
    trade(0)
    trade(1)
    for i in (0, 1):
        ring_a.send(0, 1, (0, i))
        ring_a.send(1, 1, (0, 1 - i))
    for t in range(tp):
        for place, ref in ((0, x_late), (ce, x_early)):
            v = ref[t * ce:(t + 1) * ce].astype(F32)
            v = (v * unit_scale(v) * pre_gain[...]).astype(BF16)
            for block in range(m.fs):
                xout[m.g, t, block, place:place + ce] = v[:, columns(block)]
    for i in range(3):
        wout[i, f] = weight(m.g, i)[...]
    xs = {o: cp.push(xout.at[m.g, m.k], xout.at[m.g, m.k], m.peer(o)) for o in range(n)}
    trade(2)
    mine = pl.ds(pl.multiple_of(m.k * ce, ce), ce)
    v = 0.5 * cot[mine].astype(F32) * post_gain[...]
    for block in range(m.fs):
        dpost[block] = v[:, columns(block)]
    for e in range(1, fy):
        back = (fy - e) % fy
        for i in (0, 1):
            ys[back, i].wait_recv()
        for i in (0, 1):
            ring_a.send(0, 1, (e, i))
            ring_a.send(1, 1, (e, 1 - i))
    for i in (0, 1):
        ring_a.arrive(0, 1, (0, i))
        ring_a.arrive(1, 1, (0, 1 - i))
    passed = []

    def spread(copies, out):
        for o in copies:
            copies[o].wait_recv()
            src = m.index(o, -1)
            for j in range(1, tp):
                passed.append(cp.push(out.at[src, m.k], out.at[src, m.k], m.sibling(j)))

    spread(xs, xout)
    ring_a.step(1)
    for e in range(fy):
        if e:
            ys[(fy - e) % fy, 2].wait_recv()
        for d in (0, 1):
            ring_b.send(d, 1, (e, 2))
    for copy in passed:
        copy.wait()
    passed.clear()

    gate[...] = jnp.zeros_like(gate)
    up[...] = jnp.zeros_like(up)
    for dist, s, ds in stages(m):
        for d in ds:
            ring_a.step(s, (d,))
        zt = m.along(dist)
        for e in range(fy):
            block = zt * fy + e

            def add(i, carry, block=block):
                rows = flat(xout[i, :, block])
                gate[i] += dot(rows, wout[0, block], 1, 0)
                up[i] += dot(rows, wout[1, block], 1, 0)
                return carry

            lax.fori_loop(0, m.G, add, 0)

    def activate(i, carry):
        v = gate[i]
        hid[i] = (v * (1.0 / (1.0 + jnp.exp(-v))) * up[i]).astype(BF16)
        return carry

    lax.fori_loop(0, m.G, activate, 0)
    for t in range(tp):
        hout[m.z, t] = hid[:, (2 * t + 1) * ce:(2 * t + 2) * ce]
    ring_h = Ring(m, cp, lambda c: hout.at[m.z, c], lambda z, c: hout.at[z, c], list(range(tp)))

    order = stages(m)
    sc = Scatter(m, cp, p, rx, tx, rg, acc, lambda t: m.along(order[t][0]))
    for t, (dist, s, ds) in enumerate(order):
        for d in ds:
            ring_b.step(s, (d,))
        if t == len(order) - 1:
            for i in range(tp):
                for d in (0, 1):
                    ring_h.send(d, 1, ring_h.order[d][i])
        zt = m.along(dist)
        for e in range(fy):
            block = zt * fy + e

            def product(i, carry, block=block, e=e):
                p[t, e, i] = dot(hid[i], wout[2, block], 1, 1).astype(BF16).reshape(p.shape[3:])
                return carry

            lax.fori_loop(0, m.G, product, 0)
        sc.start(t)
        if t:
            sc.middle(t - 1)
    sc.middle(len(order) - 1)
    for t in range(len(order)):
        sc.end(t)
    places = [divmod(block, fy) for block in range(m.fs)]

    def row_sum(term):
        return sum(jnp.sum(term(*place), axis=-1, keepdims=True) for place in places)

    rz = lax.rsqrt(row_sum(lambda t, e: acc[t, e, ce:] * acc[t, e, ce:]) / D + eps)
    mix = row_sum(lambda t, e: acc[t, e, ce:] * dpost[t * fy + e]) / D
    factor = rz * rz * mix
    for t, e in places:
        dall[m.g, m.k, t * fy + e] = (rz * (dpost[t * fy + e] - acc[t, e, ce:] * factor)).astype(BF16)
    dg = {o: cp.push(dall.at[m.g, m.k], dall.at[m.g, m.k], m.peer(o)) for o in range(n)}
    own = [cp.push(dall.at[m.g, m.k], dall.at[m.g, m.k], m.sibling(j)) for j in range(1, tp)]
    across = {}
    for s in range(1, fz):
        src = dall.at[m.g, m.k, pl.ds(m.along(s) * fy, fy)]
        across[s] = cp.push(src, dz.at[m.z, m.k, m.g], m.level(s))
    dz[m.z, m.k, m.g] = dall[m.g, m.k, pl.ds(m.z * fy, fy)]
    late_rz = lax.rsqrt(row_sum(lambda t, e: acc[t, e, :ce] * acc[t, e, :ce]) / D + eps)
    for t, e in places:
        cols = columns(t * fy + e)
        v = 0.5 * acc[t, e, :ce] * late_rz * post_gain[:, cols]
        y_out[m.k, :, cols] = (x_late[mine, cols].astype(F32) + v).astype(BF16)
    spread(dg, dall)
    late = [cp.push(y_out.at[m.k], y_out.at[m.k], m.sibling(j)) for j in range(1, tp)]
    ring_h.step(1)
    for copy in passed + own:
        copy.wait()
    passed.clear()

    def back(i, carry):
        total = dot(flat(dall[i, :, 0]), wout[2, 0], 1, 0)
        for block in range(1, m.fs):
            total = total + dot(flat(dall[i, :, block]), wout[2, block], 1, 0)
        dhid[i] = total
        return carry

    lax.fori_loop(0, m.G, back, 0)

    def gates(i, carry):
        for t in range(tp):
            its, to = pl.ds((2 * t + 1) * ce, ce), pl.ds(t * ce, ce)
            g, dh = gate[i, its], dhid[i, to]
            sig = 1.0 / (1.0 + jnp.exp(-g))
            dgate[i, to] = (dh * up[i, its] * sig * (1.0 + g * (1.0 - sig))).astype(BF16)
            dup[i, to] = (dh * g * sig).astype(BF16)
        return carry

    lax.fori_loop(0, m.G, gates, 0)
    for s in across:
        across[s].wait_recv()
    feats = {o: cp.push(dz.at[:, m.k, m.g], dz.at[:, m.k, m.g], m.peer(o)) for o in range(n)}
    dsc = Scatter(m, cp, q, qx, qt, qg, dacc, lambda t: t)
    for t in range(fz):
        for e in range(fy):
            block = t * fy + e

            def terms(i, carry, block=block, e=e, t=t):
                v = dot(dgate[i], wout[0, block], 1, 1) + dot(dup[i], wout[1, block], 1, 1)
                q[t, e, i] = v.astype(BF16).reshape(q.shape[3:])
                return carry

            lax.fori_loop(0, m.G, terms, 0)
        dsc.start(t)
        if t:
            dsc.middle(t - 1)
    dsc.middle(fz - 1)
    for s in range(2, ring_h.half + 1):
        ring_h.step(s)
    for o in range(n):
        feats[o].wait_recv()
    passed += [cp.push(dz.at[:, m.k], dz.at[:, m.k], m.sibling(j)) for j in range(1, tp)]
    for t in range(fz):
        dsc.end(t)
    xf = x_early[mine].astype(F32)
    rs = unit_scale(xf)
    gained = lambda t, e: dacc[t, e] * pre_gain[:, columns(t * fy + e)]
    mix = row_sum(lambda t, e: gained(t, e) * xf[:, columns(t * fy + e)]) / D
    factor = rs * rs * mix
    for t, e in places:
        cols = columns(t * fy + e)
        v = rs * (gained(t, e) - xf[:, cols] * factor)
        dx_out[m.k, :, cols] = (cot[mine, cols].astype(F32) + v).astype(BF16)
    last = [cp.push(dx_out.at[m.k], dx_out.at[m.k], m.sibling(j)) for j in range(1, tp)]
    for copy in passed:
        copy.wait()
    sends = []

    def gradient(r, e):
        a = dz[:, :, pl.ds(r * fy, fy), e]
        b = hout[:, :, pl.ds(r * fy, fy)]
        return dot(flat(a), flat(b), 0, 0).astype(BF16)

    for o in range(n):
        r, y = m.moved(o)
        dw[o] = gradient(r, y)
        sends.append(cp.push(dw.at[o], owned_at(m.g), m.peer(o)))
    owned_at(m.g)[...] = gradient(m.r, m.y)
    for copy in sends + last + late:
        copy.wait()
    for copies in (xs, ys, dg, across, feats):
        for copy in copies.values():
            copy.wait_send()
    for thing in (ring_a, ring_b, ring_h, sc, dsc):
        thing.finish()


def body(sizes, x_late, x_early, cotangent, pre_gain, post_gain, gate_weight, up_weight, down_weight,
         down_grad_sum):
    R, fs, tp = sizes
    fy = 2
    fz, G = fs // fy, R * fy
    rows, D = x_late.shape
    drows, width = gate_weight.shape
    part = width // G
    n = G - 1
    ce = rows // tp
    c = 2 * ce
    S, V = jax.ShapeDtypeStruct, pltpu.VMEM

    weights = [gate_weight, up_weight, down_weight]
    aligned = part % 128 == 0
    if not aligned:
        weights = [jnp.stack([w.reshape(drows, G, part) for w in weights]).transpose(2, 0, 1, 3)]
    ring = 2 * (fz // 2)
    count = (3 * (fy - 1) + ring * (3 * fy + tp) + 2 * (n + n * (tp - 1)) + 3 * (tp - 1)
             + 2 * fz * (tp - 1 + n) + fz - 1 + n + tp - 1 + n)

    def scatter(c):
        return [
            V((fz, fy, G, tp, c, drows), BF16),
            V((tp - 1, fz, fy, G, c, drows), BF16),
            V((fz, n, fy, c, drows), BF16),
            V((fz, n, fy, c, drows), BF16),
            V((fz, fy, c, drows), F32),
        ]

    all_rows, early_rows = tp * c, tp * ce
    y_late, dx_early, owned = pl.pallas_call(
        functools.partial(kernel, sizes, D, len(weights)),
        out_shape=[
            S((tp, ce, D), BF16), S((tp, ce, D), BF16),
            S((drows, width) if aligned else (G, drows, part), BF16),
        ],
        in_specs=[VMEM] * (len(weights) + 5),
        out_specs=[VMEM] * 3,
        scratch_shapes=[
            V((3, fs, drows, part), BF16),
            V((G, tp, fs, c, drows), BF16),
            V((fs, ce, drows), F32),
            V((G, all_rows, part), F32),
            V((G, all_rows, part), F32),
            V((G, all_rows, part), BF16),
            V((fz, tp, G, ce, part), BF16),
        ] + scatter(c) + [
            V((G, tp, fs, ce, drows), BF16),
            V((G, early_rows, part), F32),
            V((G, early_rows, part), BF16),
            V((G, early_rows, part), BF16),
            V((fz, tp, G, fy, ce, drows), BF16),
        ] + scatter(ce) + [
            V((n, drows, part), BF16),
            DMA((2, count)),
        ],
        compiler_params=pltpu.CompilerParams(
            collective_id=0, has_side_effects=True, vmem_limit_bytes=60 * 1024 * 1024
        ),
    )(*weights, x_late, x_early, cotangent, pre_gain.reshape(1, D), post_gain.reshape(1, D))
    if not aligned:
        owned = owned.transpose(1, 0, 2).reshape(drows, width)
    down_grad_out = down_grad_sum + owned.astype(F32)
    return (y_late.reshape(rows, D), dx_early.reshape(rows, D), down_grad_out)


def solution(mesh):
    sizes = tuple(mesh.shape[a] for a in ("rep", "fs", "tp"))
    in_specs = (
        P(("rep", "fs"), None),
        P(("rep", "fs"), None),
        P(("rep", "fs"), None),
        P(),
        P(),
        P("fs", "tp"),
        P("fs", "tp"),
        P("fs", "tp"),
        P(("rep", "fs"), "tp"),
    )
    out_specs = (P(("rep", "fs"), None), P(("rep", "fs"), None), P(("rep", "fs"), "tp"))
    return jax.shard_map(
        functools.partial(body, sizes), mesh=mesh, in_specs=in_specs, out_specs=out_specs, check_vma=False
    )
```

```python
import functools
import itertools

import jax
import jax.numpy as jnp
from jax import lax
from jax.experimental import pallas as pl
from jax.experimental.pallas import tpu as pltpu
from jax.sharding import PartitionSpec as P

eps = 1e-06
F32, BF16 = jnp.float32, jnp.bfloat16
VMEM = pl.BlockSpec(memory_space=pltpu.VMEM)
DMA = pltpu.SemaphoreType.DMA


class Grid:
    def __init__(self, sizes):
        self.R, self.fs, self.tp = sizes
        self.fy = 2
        self.fz = self.fs // self.fy
        self.G = self.R * self.fy
        self.offsets = list(itertools.product(range(self.R), range(self.fy)))[1:]
        self.r, f, self.k = (lax.axis_index(n) for n in ("rep", "fs", "tp"))
        self.z, self.y = lax.div(f, self.fy), lax.rem(f, self.fy)
        self.g = self.r * self.fy + self.y

    def moved(self, o, sign=1):
        dr, dy = self.offsets[o]
        r = lax.rem(self.r + self.R + sign * dr, self.R)
        y = lax.rem(self.y + self.fy + sign * dy, self.fy)
        return r, y

    def index(self, o, sign=1):
        r, y = self.moved(o, sign)
        return r * self.fy + y

    def peer(self, o):
        r, y = self.moved(o)
        return {"rep": r, "fs": self.z * self.fy + y, "tp": self.k}

    def sibling_index(self, j):
        return lax.rem(self.k + j, self.tp)

    def sibling(self, j):
        return {"rep": self.r, "fs": self.z * self.fy + self.y, "tp": self.sibling_index(j)}

    def along(self, step):
        return lax.rem(self.z + self.fz + step, self.fz)

    def level(self, step):
        return {"rep": self.r, "fs": self.along(step) * self.fy + self.y, "tp": self.k}

    def barrier(self, group=False, pair=False, ring=False, levels=False):
        sem = pltpu.get_barrier_semaphore()
        targets = []
        if group:
            targets += [self.peer(o) for o in range(len(self.offsets))]
        if pair:
            targets += [self.sibling(j) for j in range(1, self.tp)]
        if levels:
            targets += [self.level(s) for s in range(1, self.fz)]
        elif ring:
            targets += [self.level(1), self.level(-1)]
        for t in targets:
            pl.semaphore_signal(sem, inc=1, device_id=t, device_id_type=pl.DeviceIdType.MESH)
        pl.semaphore_wait(sem, len(targets))


class Copies:
    def __init__(self, sems):
        self.sems, self.used = sems, 0

    def push(self, src, dst, to):
        copy = pltpu.make_async_remote_copy(
            src_ref=src, dst_ref=dst, send_sem=self.sems.at[0, self.used], recv_sem=self.sems.at[1, self.used],
            device_id=to, device_id_type=pl.DeviceIdType.MESH,
        )
        self.used += 1
        copy.start()
        return copy


class Ring:
    def __init__(self, m, cp, first, slot, chunks):
        self.m, self.cp, self.first, self.slot = m, cp, first, slot
        self.order = {0: chunks, 1: chunks[len(chunks) // 2:] + chunks[:len(chunks) // 2]}
        self.fronts = {0: set(chunks[: len(chunks) // 2]), 1: set(chunks[len(chunks) // 2:])}
        self.half = m.fz // 2
        self.sent, self.arrived = {}, set()

    def send(self, d, s, c):
        sign = 1 if d == 0 else -1
        block = self.m.along(-sign * (s - 1))
        src = self.first(c) if s == 1 else self.slot(block, c)
        self.sent[d, s, c] = self.cp.push(src, self.slot(block, c), self.m.level(sign))

    def arrive(self, d, s, c):
        if (d, s, c) not in self.sent or (d, s, c) in self.arrived:
            return
        self.sent[d, s, c].wait_recv()
        self.arrived.add((d, s, c))
        if s + 1 < self.half or (s + 1 == self.half and c in self.fronts[d]):
            self.send(d, s + 1, c)

    def step(self, s, ds=(0, 1)):
        for i in range(len(self.order[0])):
            for d in ds:
                self.arrive(d, s, self.order[d][i])

    def finish(self):
        for copy in self.sent.values():
            copy.wait_send()


def stages(m):
    half = m.fz // 2
    out = [(0, 0, ())]
    for s in range(1, half):
        out += [(-s, s, (0,)), (s, s, (1,))]
    return out + [(half, half, (0, 1))]


class Scatter:
    def __init__(self, m, cp, p, rx, tx, rg, acc, place):
        self.m, self.cp, self.p, self.rx, self.tx, self.rg, self.acc = m, cp, p, rx, tx, rg, acc
        self.place = place
        self.pair, self.far = {}, {}

    def start(self, t):
        m = self.m
        for j in range(1, m.tp):
            src = self.p.at[t, :, :, m.sibling_index(j)]
            self.pair[t, j] = self.cp.push(src, self.rx.at[j - 1, t], m.sibling(j))

    def middle(self, t):
        m, n = self.m, len(self.m.offsets)
        for j in range(1, m.tp):
            self.pair[t, j].wait_recv()

        def total(block):
            value = self.p[t, :, block, m.k].astype(F32)
            for j in range(1, m.tp):
                value = value + self.rx[j - 1, t, :, block].astype(F32)
            return value

        for o in range(n):
            self.tx[t, o] = total(m.index(o)).astype(BF16)
            self.far[t, o] = self.cp.push(self.tx.at[t, o], self.rg.at[t, o], m.peer(o))
        self.acc[self.place(t)] = total(m.g)

    def end(self, t):
        n = len(self.m.offsets)
        for o in range(n):
            self.far[t, o].wait_recv()
        value = self.acc[self.place(t)]
        for o in range(n):
            value = value + self.rg[t, o].astype(F32)
        self.acc[self.place(t)] = value

    def finish(self):
        for copy in list(self.pair.values()) + list(self.far.values()):
            copy.wait_send()


def flat(v):
    return v.reshape(-1, v.shape[-1])


def dot(a, b, ca, cb):
    return lax.dot_general(a, b, (((ca,), (cb,)), ((), ())), preferred_element_type=F32)


def unit_scale(v):
    return lax.rsqrt(jnp.mean(v * v, axis=-1, keepdims=True) + eps)


def kernel(sizes, D, nw, *refs):
    ws, refs = refs[:nw], refs[nw:]
    (x_late, x_early, cot, pre_gain, post_gain, y_out, dx_out, owned_out,
     wout, xout, dpost, gate, up, hid, hout, p, rx, tx, rg, acc, dall, dhid, dgate, dup, dz,
           q, qx, qt, qg, dacc, dw, sems) = refs
    m = Grid(sizes)
    cp = Copies(sems)
    n, fy, tp, fz = len(m.offsets), m.fy, m.tp, m.fz
    m.barrier(group=True, pair=True, levels=True)
    f = m.z * fy + m.y
    rows, part = x_late.shape[0], wout.shape[-1]
    ce, drows = rows // tp, D // m.fs

    def weight(g, i):
        if nw == 1:
            return ws[0].at[g, i]
        return ws[i].at[:, pl.ds(pl.multiple_of(g * part, part), part)]

    def owned_at(g):
        if nw == 1:
            return owned_out.at[g]
        return owned_out.at[:, pl.ds(pl.multiple_of(g * part, part), part)]

    def columns(block):
        return slice(block * drows, (block + 1) * drows)

    def where(z, c):
        e, i = c
        return wout.at[i, z * fy + lax.rem(m.y + e, fy)]

    def first(c):
        return weight(m.g, c[1]) if c[0] == 0 else where(m.z, c)

    ys = {}

    def trade(i):
        for e in range(1, fy):
            o = m.offsets.index((0, e))
            ys[e, i] = cp.push(weight(m.index(o), i), wout.at[i, f], m.peer(o))

    ring_a = Ring(m, cp, first, where, [(e, i) for i in (0, 1) for e in range(fy)])
    ring_b = Ring(m, cp, first, where, [(e, 2) for e in range(fy)])
    trade(0)
    trade(1)
    for i in (0, 1):
        ring_a.send(0, 1, (0, i))
        ring_a.send(1, 1, (0, 1 - i))
    for t in range(tp):
        for place, ref in ((0, x_late), (ce, x_early)):
            v = ref[t * ce:(t + 1) * ce].astype(F32)
            v = (v * unit_scale(v) * pre_gain[...]).astype(BF16)
            for block in range(m.fs):
                xout[m.g, t, block, place:place + ce] = v[:, columns(block)]
    for i in range(3):
        wout[i, f] = weight(m.g, i)[...]
    xs = {o: cp.push(xout.at[m.g, m.k], xout.at[m.g, m.k], m.peer(o)) for o in range(n)}
    trade(2)
    mine = pl.ds(pl.multiple_of(m.k * ce, ce), ce)
    v = 0.5 * cot[mine].astype(F32) * post_gain[...]
    for block in range(m.fs):
        dpost[block] = v[:, columns(block)]
    for e in range(1, fy):
        back = (fy - e) % fy
        for i in (0, 1):
            ys[back, i].wait_recv()
        for i in (0, 1):
            ring_a.send(0, 1, (e, i))
            ring_a.send(1, 1, (e, 1 - i))
    for i in (0, 1):
        ring_a.arrive(0, 1, (0, i))
        ring_a.arrive(1, 1, (0, 1 - i))
    passed = []

    def spread(copies, out):
        for o in copies:
            copies[o].wait_recv()
            src = m.index(o, -1)
            for j in range(1, tp):
                passed.append(cp.push(out.at[src, m.k], out.at[src, m.k], m.sibling(j)))

    spread(xs, xout)
    ring_a.step(1)
    for e in range(fy):
        if e:
            ys[(fy - e) % fy, 2].wait_recv()
        for d in (0, 1):
            ring_b.send(d, 1, (e, 2))
    for copy in passed:
        copy.wait()
    passed.clear()

    gate[...] = jnp.zeros_like(gate)
    up[...] = jnp.zeros_like(up)
    for dist, s, ds in stages(m):
        for d in ds:
            ring_a.step(s, (d,))
        zt = m.along(dist)
        for e in range(fy):
            block = zt * fy + e

            def add(i, carry, block=block):
                rows = flat(xout[i, :, block])
                gate[i] += dot(rows, wout[0, block], 1, 0)
                up[i] += dot(rows, wout[1, block], 1, 0)
                return carry

            lax.fori_loop(0, m.G, add, 0)

    def activate(i, carry):
        v = gate[i]
        hid[i] = (v * (1.0 / (1.0 + jnp.exp(-v))) * up[i]).astype(BF16)
        return carry

    lax.fori_loop(0, m.G, activate, 0)
    for t in range(tp):
        hout[m.z, t] = hid[:, (2 * t + 1) * ce:(2 * t + 2) * ce]
    ring_h = Ring(m, cp, lambda c: hout.at[m.z, c], lambda z, c: hout.at[z, c], list(range(tp)))

    order = stages(m)
    sc = Scatter(m, cp, p, rx, tx, rg, acc, lambda t: m.along(order[t][0]))
    for t, (dist, s, ds) in enumerate(order):
        for d in ds:
            ring_b.step(s, (d,))
        if t == len(order) - 1:
            for i in range(tp // 2):
                for d in (0, 1):
                    ring_h.send(d, 1, ring_h.order[d][i])
        zt = m.along(dist)
        for e in range(fy):
            block = zt * fy + e

            def product(i, carry, block=block, e=e):
                p[t, e, i] = dot(hid[i], wout[2, block], 1, 1).astype(BF16).reshape(p.shape[3:])
                return carry

            lax.fori_loop(0, m.G, product, 0)
        sc.start(t)
        if t:
            sc.middle(t - 1)
    sc.middle(len(order) - 1)
    for t in range(len(order)):
        sc.end(t)
    places = [divmod(block, fy) for block in range(m.fs)]

    def row_sum(term):
        return sum(jnp.sum(term(*place), axis=-1, keepdims=True) for place in places)

    rz = lax.rsqrt(row_sum(lambda t, e: acc[t, e, ce:] * acc[t, e, ce:]) / D + eps)
    mix = row_sum(lambda t, e: acc[t, e, ce:] * dpost[t * fy + e]) / D
    factor = rz * rz * mix
    for t, e in places:
        dall[m.g, m.k, t * fy + e] = (rz * (dpost[t * fy + e] - acc[t, e, ce:] * factor)).astype(BF16)
    dg = {o: cp.push(dall.at[m.g, m.k], dall.at[m.g, m.k], m.peer(o)) for o in range(n)}
    own = [cp.push(dall.at[m.g, m.k], dall.at[m.g, m.k], m.sibling(j)) for j in range(1, tp)]
    across = {}
    for s in range(1, fz):
        src = dall.at[m.g, m.k, pl.ds(m.along(s) * fy, fy)]
        across[s] = cp.push(src, dz.at[m.z, m.k, m.g], m.level(s))
    for i in range(tp // 2, tp):
        for d in (0, 1):
            ring_h.send(d, 1, ring_h.order[d][i])
    dz[m.z, m.k, m.g] = dall[m.g, m.k, pl.ds(m.z * fy, fy)]
    late_rz = lax.rsqrt(row_sum(lambda t, e: acc[t, e, :ce] * acc[t, e, :ce]) / D + eps)
    for t, e in places:
        cols = columns(t * fy + e)
        v = 0.5 * acc[t, e, :ce] * late_rz * post_gain[:, cols]
        y_out[m.k, :, cols] = (x_late[mine, cols].astype(F32) + v).astype(BF16)
    spread(dg, dall)
    late = [cp.push(y_out.at[m.k], y_out.at[m.k], m.sibling(j)) for j in range(1, tp)]
    for copy in passed + own:
        copy.wait()
    passed.clear()
    for s in across:
        across[s].wait_recv()
    feats = {o: cp.push(dz.at[:, m.k, m.g], dz.at[:, m.k, m.g], m.peer(o)) for o in range(n)}
    for i in range(tp // 2):
        for d in (0, 1):
            ring_h.arrive(d, 1, ring_h.order[d][i])

    def back(i, carry):
        total = dot(flat(dall[i, :, 0]), wout[2, 0], 1, 0)
        for block in range(1, m.fs):
            total = total + dot(flat(dall[i, :, block]), wout[2, block], 1, 0)
        dhid[i] = total
        return carry

    lax.fori_loop(0, m.G, back, 0)

    def gates(i, carry):
        for t in range(tp):
            its, to = pl.ds((2 * t + 1) * ce, ce), pl.ds(t * ce, ce)
            g, dh = gate[i, its], dhid[i, to]
            sig = 1.0 / (1.0 + jnp.exp(-g))
            dgate[i, to] = (dh * up[i, its] * sig * (1.0 + g * (1.0 - sig))).astype(BF16)
            dup[i, to] = (dh * g * sig).astype(BF16)
        return carry

    lax.fori_loop(0, m.G, gates, 0)
    ring_h.step(1)
    dsc = Scatter(m, cp, q, qx, qt, qg, dacc, lambda t: t)
    for t in range(fz):
        for e in range(fy):
            block = t * fy + e

            def terms(i, carry, block=block, e=e, t=t):
                v = dot(dgate[i], wout[0, block], 1, 1) + dot(dup[i], wout[1, block], 1, 1)
                q[t, e, i] = v.astype(BF16).reshape(q.shape[3:])
                return carry

            lax.fori_loop(0, m.G, terms, 0)
        dsc.start(t)
        if t:
            dsc.middle(t - 1)
    dsc.middle(fz - 1)
    for s in range(2, ring_h.half + 1):
        ring_h.step(s)
    for o in range(n):
        feats[o].wait_recv()
    passed += [cp.push(dz.at[:, m.k], dz.at[:, m.k], m.sibling(j)) for j in range(1, tp)]
    for copy in passed:
        copy.wait()
    sends = []

    def gradient(r, e):
        a = dz[:, :, pl.ds(r * fy, fy), e]
        b = hout[:, :, pl.ds(r * fy, fy)]
        return dot(flat(a), flat(b), 0, 0).astype(BF16)

    for o in range(n):
        r, y = m.moved(o)
        dw[o] = gradient(r, y)
        sends.append(cp.push(dw.at[o], owned_at(m.g), m.peer(o)))
    owned_at(m.g)[...] = gradient(m.r, m.y)
    for t in range(fz):
        dsc.end(t)
    xf = x_early[mine].astype(F32)
    rs = unit_scale(xf)
    gained = lambda t, e: dacc[t, e] * pre_gain[:, columns(t * fy + e)]
    mix = row_sum(lambda t, e: gained(t, e) * xf[:, columns(t * fy + e)]) / D
    factor = rs * rs * mix
    for t, e in places:
        cols = columns(t * fy + e)
        v = rs * (gained(t, e) - xf[:, cols] * factor)
        dx_out[m.k, :, cols] = (cot[mine, cols].astype(F32) + v).astype(BF16)
    last = [cp.push(dx_out.at[m.k], dx_out.at[m.k], m.sibling(j)) for j in range(1, tp)]
    for copy in sends + last + late:
        copy.wait()
    for copies in (xs, ys, dg, across, feats):
        for copy in copies.values():
            copy.wait_send()
    for thing in (ring_a, ring_b, ring_h, sc, dsc):
        thing.finish()


def body(sizes, x_late, x_early, cotangent, pre_gain, post_gain, gate_weight, up_weight, down_weight,
         down_grad_sum):
    R, fs, tp = sizes
    fy = 2
    fz, G = fs // fy, R * fy
    rows, D = x_late.shape
    drows, width = gate_weight.shape
    part = width // G
    n = G - 1
    ce = rows // tp
    c = 2 * ce
    S, V = jax.ShapeDtypeStruct, pltpu.VMEM

    weights = [gate_weight, up_weight, down_weight]
    aligned = part % 128 == 0
    if not aligned:
        weights = [jnp.stack([w.reshape(drows, G, part) for w in weights]).transpose(2, 0, 1, 3)]
    ring = 2 * (fz // 2)
    count = (3 * (fy - 1) + ring * (3 * fy + tp) + 2 * (n + n * (tp - 1)) + 3 * (tp - 1)
             + 2 * fz * (tp - 1 + n) + fz - 1 + n + tp - 1 + n)

    def scatter(c):
        return [
            V((fz, fy, G, tp, c, drows), BF16),
            V((tp - 1, fz, fy, G, c, drows), BF16),
            V((fz, n, fy, c, drows), BF16),
            V((fz, n, fy, c, drows), BF16),
            V((fz, fy, c, drows), F32),
        ]

    all_rows, early_rows = tp * c, tp * ce
    y_late, dx_early, owned = pl.pallas_call(
        functools.partial(kernel, sizes, D, len(weights)),
        out_shape=[
            S((tp, ce, D), BF16), S((tp, ce, D), BF16),
            S((drows, width) if aligned else (G, drows, part), BF16),
        ],
        in_specs=[VMEM] * (len(weights) + 5),
        out_specs=[VMEM] * 3,
        scratch_shapes=[
            V((3, fs, drows, part), BF16),
            V((G, tp, fs, c, drows), BF16),
            V((fs, ce, drows), F32),
            V((G, all_rows, part), F32),
            V((G, all_rows, part), F32),
            V((G, all_rows, part), BF16),
            V((fz, tp, G, ce, part), BF16),
        ] + scatter(c) + [
            V((G, tp, fs, ce, drows), BF16),
            V((G, early_rows, part), F32),
            V((G, early_rows, part), BF16),
            V((G, early_rows, part), BF16),
            V((fz, tp, G, fy, ce, drows), BF16),
        ] + scatter(ce) + [
            V((n, drows, part), BF16),
            DMA((2, count)),
        ],
        compiler_params=pltpu.CompilerParams(
            collective_id=0, has_side_effects=True, vmem_limit_bytes=60 * 1024 * 1024
        ),
    )(*weights, x_late, x_early, cotangent, pre_gain.reshape(1, D), post_gain.reshape(1, D))
    if not aligned:
        owned = owned.transpose(1, 0, 2).reshape(drows, width)
    down_grad_out = down_grad_sum + owned.astype(F32)
    return (y_late.reshape(rows, D), dx_early.reshape(rows, D), down_grad_out)


def solution(mesh):
    sizes = tuple(mesh.shape[a] for a in ("rep", "fs", "tp"))
    in_specs = (
        P(("rep", "fs"), None),
        P(("rep", "fs"), None),
        P(("rep", "fs"), None),
        P(),
        P(),
        P("fs", "tp"),
        P("fs", "tp"),
        P("fs", "tp"),
        P(("rep", "fs"), "tp"),
    )
    out_specs = (P(("rep", "fs"), None), P(("rep", "fs"), None), P(("rep", "fs"), "tp"))
    return jax.shard_map(
        functools.partial(body, sizes), mesh=mesh, in_specs=in_specs, out_specs=out_specs, check_vma=False
    )
```
